512 devices in a mesh: tp: 64 (over z, y), dp: 8 (over x, core).
Axes of the slice: x: 4, y: 8, z: 8, core: 2. Of those that a mesh axis runs over, the one named last changes fastest.
Arguments:
- hidden: bfloat16 [64, 4096], P(None, 'dp'), may hold values from -6 to 6
- norm_gain: float32 [2, 4096], P(None, 'dp'), may hold values from 0.1 to 1.9
- gate_weight: bfloat16 [2, 4096, 8192], P(None, 'dp', 'tp'), may hold values from -0.09375 to 0.09375
- inner_weight: bfloat16 [2, 4096, 8192], P(None, 'dp', 'tp'), may hold values from -0.09375 to 0.09375
- write_weight: bfloat16 [2, 4096, 2048], P(None, 'dp', 'tp'), may hold values from -0.09375 to 0.09375
- read_weight: bfloat16 [2, 4096, 2048], P(None, 'dp', 'tp'), may hold values from -0.09375 to 0.09375
- step_weight: bfloat16 [2, 4096, 128], P(None, 'dp'), may hold values from -0.09375 to 0.09375
- conv_inner: bfloat16 [2, 4, 8192], P(None, None, 'tp'), may hold values from -3 to 3
- conv_write: bfloat16 [2, 4, 2048], P(None, None, 'tp'), may hold values from -3 to 3
- conv_read: bfloat16 [2, 4, 2048], P(None, None, 'tp'), may hold values from -3 to 3
- step_bias: float32 [2, 128], P(None, 'tp'), may hold values from -4 to -1
- decay_log: float32 [2, 128], P(None, 'tp'), may hold values from -3 to 0.5
- skip_gain: float32 [2, 128], P(None, 'tp'), may hold values from 0.1 to 1.9
- group_gain: float32 [2, 8192], P(None, 'tp'), may hold values from 0.1 to 1.9
- out_weight: bfloat16 [2, 8192, 4096], P(None, 'tp', 'dp'), may hold values from -0.4 to 0.4
- state_inner: bfloat16 [2, 64, 3, 8192], P(None, 'dp', None, 'tp'), may hold values from -6 to 6
- state_write: bfloat16 [2, 64, 3, 2048], P(None, 'dp', None, 'tp'), may hold values from -6 to 6
- state_read: bfloat16 [2, 64, 3, 2048], P(None, 'dp', None, 'tp'), may hold values from -6 to 6
- recurrent: float32 [2, 64, 128, 64, 128], P(None, 'dp', 'tp'), may hold values from -1.2 to 1.2, as said below
Outputs:
- out_hidden: bfloat16 [64, 4096], P(None, 'dp')
- next_inner: bfloat16 [2, 64, 3, 8192], P(None, 'dp', None, 'tp')
- next_write: bfloat16 [2, 64, 3, 2048], P(None, 'dp', None, 'tp')
- next_read: bfloat16 [2, 64, 3, 2048], P(None, 'dp', None, 'tp')
- next_recurrent: float32 [2, 64, 128, 64, 128], P(None, 'dp', 'tp')
The draws below stay inside these ranges and needn't reach their ends.
Inputs may be any that keep to these rules, and one draw needn't show every extreme that they name: recurrent states of order a tenth, with scales that differ between heads.
All inputs are finite; a program needn't handle non-finite values.
Results may differ from the reference program's by a relative error of at most 0.025.
Values may be sent and summed in bfloat16 or wider, within the bound.
No kernel may reach another device: no remote copies, remote signals or barrier semaphores. Data moves between devices by JAX's collectives and lax.ppermute only.
A program may use at most 64 MiB of HBM per device.

```python
import math
import jax
import jax.numpy as jnp
from jax import lax

D = 4096
HEADS = 128
HEAD_DIM = 64
STATE_DIM = 128
GROUPS = 16
KERNEL = 4
LAYERS = 2
INNER = 8192
BATCH = 64
N_DP = 8


def draw_recurrent(key, part):
    first_key, second_key = jax.random.split(jax.random.fold_in(key, 17))
    shape = (LAYERS, BATCH, HEADS, HEAD_DIM, STATE_DIM)
    factor = jnp.exp(jax.random.uniform(first_key, (LAYERS, 1, HEADS, 1, 1), jnp.float32, math.log(0.03), math.log(0.3)))
    values = jax.random.truncated_normal(second_key, -4.0, 4.0, shape, jnp.float32)
    return (values * factor).astype(jnp.float32)


def draw_out_weight(key, part):
    sign_key, size_key, common_key, noise_key = jax.random.split(jax.random.fold_in(key, 29), 4)
    shape = (LAYERS, INNER, D)
    signs = jnp.where(jax.random.bernoulli(sign_key, 0.5, (LAYERS, INNER, 1)), 1.0, -1.0).astype(jnp.float32)
    magnitude = jax.random.uniform(size_key, (LAYERS, INNER, 1), jnp.float32, 1.0, 1.3)
    common = jax.random.truncated_normal(common_key, -4.0, 4.0, (LAYERS, 1, D), jnp.float32)
    noise = jax.random.truncated_normal(noise_key, -4.0, 4.0, shape, jnp.float32)
    values = (signs * magnitude * common + noise) / math.sqrt(INNER)
    return values.astype(jnp.bfloat16)


def shard_levels(stream_key, shape, cuts, smallest, high):
    def one(dim, parts):
        heights = jax.random.uniform(jax.random.fold_in(jax.random.fold_in(stream_key, 6), dim), (parts,), jnp.float32, smallest / len(cuts), high / len(cuts))
        return jnp.repeat(jnp.exp(heights), shape[dim] // parts).reshape((-1,) + (1,) * (len(shape) - dim - 1))

    factor_of = one(*cuts[0])
    for cut in cuts[1:]:
        factor_of = factor_of * one(*cut)
    return factor_of


def gaussian(key, extent, spread, reach, cuts=(), dtype=jnp.bfloat16):
    gain = shard_levels(key, extent, cuts, -0.22, 0.18) if cuts else 1.0
    drawn = jax.random.normal(key, extent, jnp.float32) * spread * gain
    return jnp.minimum(jnp.maximum(drawn, -reach), reach).astype(dtype)


def setup_inputs(seed: int = 0) -> dict:
    streams_of = jax.random.split(jax.random.key(seed), 20)
    return {
        "hidden": gaussian(streams_of[0], (BATCH, D), 1.0, 6.0, ((1, 8),)),
        "norm_gain": jnp.clip(1.0 + 0.18 * jax.random.normal(streams_of[1], (LAYERS, D), jnp.float32), 0.1, 1.9),
        "gate_weight": gaussian(streams_of[2], (LAYERS, D, INNER), D ** -0.5, 0.09375, ((1, 8), (2, 64))),
        "inner_weight": gaussian(streams_of[3], (LAYERS, D, INNER), D ** -0.5, 0.09375, ((1, 8), (2, 64))),
        "write_weight": gaussian(streams_of[4], (LAYERS, D, GROUPS * STATE_DIM), D ** -0.5, 0.09375, ((1, 8), (2, 64))),
        "read_weight": gaussian(streams_of[5], (LAYERS, D, GROUPS * STATE_DIM), D ** -0.5, 0.09375, ((1, 8), (2, 64))),
        "step_weight": gaussian(streams_of[6], (LAYERS, D, HEADS), D ** -0.5, 0.09375, ((1, 8),)),
        "conv_inner": gaussian(streams_of[7], (LAYERS, KERNEL, INNER), KERNEL ** -0.5, 3.0, ((2, 64),)),
        "conv_write": gaussian(streams_of[8], (LAYERS, KERNEL, GROUPS * STATE_DIM), KERNEL ** -0.5, 3.0, ((2, 64),)),
        "conv_read": gaussian(streams_of[9], (LAYERS, KERNEL, GROUPS * STATE_DIM), KERNEL ** -0.5, 3.0, ((2, 64),)),
        "step_bias": jnp.clip(-4.0 + 3.0 * jax.random.uniform(streams_of[10], (LAYERS, HEADS), jnp.float32) ** shard_levels(streams_of[10], (LAYERS, HEADS), ((1, 64),), -0.2, 0.2), -4.0, -1.0),
        "decay_log": jnp.clip(-3.0 + 3.5 * jax.random.uniform(streams_of[11], (LAYERS, HEADS), jnp.float32) ** shard_levels(streams_of[11], (LAYERS, HEADS), ((1, 64),), -0.2, 0.2), -3.0, 0.5),
        "skip_gain": jnp.clip(1.0 + 0.18 * jax.random.normal(streams_of[12], (LAYERS, HEADS), jnp.float32), 0.1, 1.9),
        "group_gain": jnp.clip(1.0 + 0.18 * jax.random.normal(streams_of[13], (LAYERS, INNER), jnp.float32), 0.1, 1.9),
        "out_weight": draw_out_weight(jax.random.fold_in(streams_of[19], 71), 0),
        "state_inner": gaussian(streams_of[15], (LAYERS, BATCH, KERNEL - 1, INNER), 1.0, 6.0, ((1, 8), (3, 64))),
        "state_write": gaussian(streams_of[16], (LAYERS, BATCH, KERNEL - 1, GROUPS * STATE_DIM), 1.0, 6.0, ((1, 8), (3, 64))),
        "state_read": gaussian(streams_of[17], (LAYERS, BATCH, KERNEL - 1, GROUPS * STATE_DIM), 1.0, 6.0, ((1, 8), (3, 64))),
        "recurrent": draw_recurrent(jax.random.fold_in(streams_of[19], 71), 0),
    }


eps = 1e-06

def project(normed, weight):
    block_rows = D // N_DP
    left_side = normed.reshape(normed.shape[0], N_DP, block_rows).astype(jnp.float32)
    right_side = weight.reshape(N_DP, block_rows, weight.shape[1]).astype(jnp.float32)
    pieces = jnp.einsum('bkr,krc->kbc', left_side, right_side)
    pieces = lax.optimization_barrier(pieces.astype(jnp.bfloat16)).astype(jnp.float32)
    return lax.optimization_barrier(jnp.sum(pieces, axis=0)).astype(jnp.bfloat16)

def convolve(state, fresh_row, kernel):
    window = jnp.concatenate([state, fresh_row[:, None, :]], axis=1)
    summed = lax.optimization_barrier(jnp.sum(window.astype(jnp.float32) * kernel.astype(jnp.float32)[None], axis=1))
    return (jax.nn.silu(summed), window[:, 1:])

def mixer_block(stream, number, norm_gain, gate_weight, inner_weight, write_weight, read_weight, step_weight, conv_inner, conv_write, conv_read, step_bias, decay_log, skip_gain, group_gain, out_weight, state_inner, state_write, state_read, recurrent):
    wide_in = stream.astype(jnp.float32)
    factor = lax.rsqrt(lax.optimization_barrier(jnp.mean(wide_in * wide_in, axis=1, keepdims=True)) + eps)
    normed = (wide_in * factor * norm_gain[number][None, :]).astype(jnp.bfloat16)
    gate_raw = project(normed, gate_weight[number])
    inner_raw = project(normed, inner_weight[number])
    write_raw = project(normed, write_weight[number])
    read_raw = project(normed, read_weight[number])
    step_raw = project(normed, step_weight[number])
    inner_act, next_inner = convolve(state_inner[number], inner_raw, conv_inner[number])
    write_act, next_write = convolve(state_write[number], write_raw, conv_write[number])
    read_act, next_read = convolve(state_read[number], read_raw, conv_read[number])
    write_act = write_act.astype(jnp.bfloat16)
    read_act = read_act.astype(jnp.bfloat16)
    rows_here = stream.shape[0]
    per_group = HEADS // GROUPS
    write_groups = jnp.transpose(write_act.reshape(rows_here, STATE_DIM, GROUPS), (0, 2, 1))
    read_groups = jnp.transpose(read_act.reshape(rows_here, STATE_DIM, GROUPS), (0, 2, 1))
    write_vec = jnp.repeat(write_groups, per_group, axis=1).astype(jnp.float32)
    read_vec = jnp.repeat(read_groups, per_group, axis=1).astype(jnp.float32)
    step_size = jax.nn.softplus(step_raw.astype(jnp.float32) + step_bias[number][None, :])
    retain = jnp.exp(-step_size * jnp.exp(decay_log[number])[None, :])
    inner_heads = inner_act.reshape(rows_here, HEADS, HEAD_DIM)
    updated = retain[:, :, None, None] * recurrent[number] + (step_size[:, :, None] * inner_heads)[:, :, :, None] * write_vec[:, :, None, :]
    readout = jnp.einsum('bhpn,bhn->bhp', updated, read_vec, precision=lax.Precision.HIGHEST)
    readout = readout + skip_gain[number][None, :, None] * inner_heads
    gated_out = readout.reshape(rows_here, INNER) * jax.nn.silu(gate_raw.astype(jnp.float32))
    grouped = gated_out.reshape(rows_here, GROUPS, INNER // GROUPS)
    group_factor = lax.rsqrt(lax.optimization_barrier(jnp.mean(grouped * grouped, axis=2, keepdims=True)) + eps)
    group_normed = ((grouped * group_factor).reshape(rows_here, INNER) * group_gain[number][None, :]).astype(jnp.bfloat16)
    branch = jnp.dot(group_normed, out_weight[number], preferred_element_type=jnp.float32)
    result = (wide_in + branch).astype(jnp.bfloat16)
    return (result, next_inner, next_write, next_read, updated)

def reference(hidden, norm_gain, gate_weight, inner_weight, write_weight, read_weight, step_weight, conv_inner, conv_write, conv_read, step_bias, decay_log, skip_gain, group_gain, out_weight, state_inner, state_write, state_read, recurrent):
    stream = hidden
    collected = [[], [], [], []]
    for number in range(LAYERS):
        outcome = mixer_block(stream, number, norm_gain, gate_weight, inner_weight, write_weight, read_weight, step_weight, conv_inner, conv_write, conv_read, step_bias, decay_log, skip_gain, group_gain, out_weight, state_inner, state_write, state_read, recurrent)
        stream = outcome[0]
        for position in range(4):
            collected[position].append(outcome[position + 1])
    return (stream, jnp.stack(collected[0]), jnp.stack(collected[1]), jnp.stack(collected[2]), jnp.stack(collected[3]))
```

```python
import jax
import jax.numpy as jnp
from jax import lax
from jax.sharding import Mesh
from jax.sharding import PartitionSpec as P

D = 4096
HEADS = 128
GROUPS = 16
DP = ("dp_0", "dp_1")
TP = ("tp_0", "tp_1")
Y = "tp_1"
Z = "tp_0"
YD = ("tp_1", "dp_0", "dp_1")
EPS = 1e-06
BF = jnp.bfloat16
F32 = jnp.float32


def exchange(pieces, axis):
    return lax.all_to_all(pieces, axis, 0, 0, tiled=True)


def to_each(shard, axis):
    return exchange(jnp.broadcast_to(shard[None], (lax.axis_size(axis), *shard.shape)), axis)


def split_two(wide):
    high = lax.reduce_precision(wide, 8, 7)
    return high.astype(BF), (wide - high).astype(BF)


def dot(a, b):
    return jnp.dot(a, b, preferred_element_type=F32)


def unshuffle():
    row = jnp.arange(256)[:, None]
    col = jnp.arange(256)[None, :]
    return (row == (col % 128) // 2 * 4 + col // 128 * 2 + col % 2).astype(BF)


def conv(rows, fresh, taps):
    taps = taps.astype(F32)
    total = fresh.astype(F32) * taps[3][None]
    for k in range(3):
        total = total + rows[:, k].astype(F32) * taps[k][None]
    return jax.nn.silu(total)


def shifted(rows, fresh):
    return jnp.concatenate([rows[:, 1:], fresh[:, None]], axis=1)


def mix(raw, step_raw, inner_act, vectors, bias, decay, skip, recurrent):
    write_vec, read_vec = vectors[0], vectors[1]
    step = jax.nn.softplus(step_raw.astype(F32) + bias[None, :])
    retain = jnp.exp(-step * jnp.exp(decay)[None, :])
    heads = inner_act.reshape(8, 2, 64)
    updated = (
        retain[:, :, None, None] * recurrent
        + (step[:, :, None] * heads)[:, :, :, None] * write_vec[:, None, None, :]
    )
    readout = jnp.sum(updated * read_vec[:, None, None, :], axis=3)
    readout = readout + skip[None, :, None] * heads
    gated = readout.reshape(8, 128) * jax.nn.silu(raw.astype(F32))
    return updated, gated.astype(BF)


def local(
    hidden,
    norm_gain,
    gate_weight,
    inner_weight,
    write_weight,
    read_weight,
    step_weight,
    conv_inner,
    conv_write,
    conv_read,
    step_bias,
    decay_log,
    skip_gain,
    group_gain,
    out_weight,
    state_inner,
    state_write,
    state_read,
    recurrent,
):
    t = lax.axis_index(TP)

    by_feature = out_weight.reshape(2, 128, 8, 64)
    moved = jnp.concatenate([by_feature[0], by_feature[1]], axis=2)
    moved = jnp.moveaxis(moved, 1, 0)
    gain_high, gain_low = split_two(group_gain)
    gains = jnp.stack([gain_high[0], gain_low[0], gain_high[1], gain_low[1]])
    gains = jnp.concatenate([gains, jnp.zeros((4, 128), BF)], axis=0)
    moved = jnp.concatenate([moved, jnp.broadcast_to(gains[None], (8, 8, 128))], axis=1)
    slab = exchange(moved, Y)

    def channel_rows(weight, taps, rows):
        return jnp.concatenate(
            [weight[1].T, taps[1].T, rows[1].reshape(24, 32).T, jnp.zeros((32, 92), BF)], axis=1
        )

    later = jnp.stack(
        [
            channel_rows(write_weight, conv_write, state_write),
            channel_rows(read_weight, conv_read, state_read),
        ]
    )

    def project(wide, number, extra):
        scaled = (wide * norm_gain[number][None, :]).astype(BF)
        squares = jnp.sum(wide * wide, axis=1, keepdims=True)
        high, low = split_two(squares)
        step_own = lax.dynamic_slice_in_dim(step_weight[number], 2 * t, 2, 1)
        parts = [
            dot(scaled, gate_weight[number]).astype(BF),
            dot(scaled, inner_weight[number]).astype(BF),
            dot(scaled, write_weight[number]).astype(BF),
            dot(scaled, read_weight[number]).astype(BF),
            dot(scaled, step_own).astype(BF),
            high,
            low,
            jnp.zeros((64, 60), BF),
        ]
        if extra is not None:
            parts.append(
                lax.dot_general(
                    scaled, extra, (((1,), (1,)), ((), ())), preferred_element_type=F32
                ).astype(BF)
            )
        both = jnp.concatenate(parts, axis=1)
        got = exchange(both.reshape(8, 8, -1), DP)
        total = jnp.sum(got.astype(F32), axis=0)
        factor = lax.rsqrt((total[:, 322:323] + total[:, 323:324]) / D + EPS)
        return (total * factor).astype(BF)

    def finish(gated, number, own):
        got = to_each(gated, YD).reshape(8, 64, 128).astype(F32)
        squares = jnp.sum(got * got, axis=2)
        group = jnp.sum(squares.reshape(2, 4, 64), axis=1)
        factor = lax.rsqrt(group / 512 + EPS)
        factor = jnp.broadcast_to(factor[:, None], (2, 4, 64)).reshape(8, 64)
        gain = slab[:, 128 + 2 * number].astype(F32) + slab[:, 129 + 2 * number].astype(F32)
        normed = (got * factor[:, :, None] * gain[:, None, :]).astype(BF)
        normed = jnp.moveaxis(normed, 0, 1).reshape(64, 1024)
        weight = slab[:, :128, 64 * number : 64 * number + 64].reshape(1024, 64)
        part = dot(normed, weight).astype(BF)
        part = jnp.concatenate([part[:32], part[32:]], axis=1)
        pieces = to_each(part, Z)
        own = (own.astype(F32) + jnp.sum(pieces.astype(F32), axis=0)).astype(BF)
        blocks = to_each(own, Y)
        blocks = jnp.concatenate([blocks[:, :, :64], blocks[:, :, 64:]], axis=1)
        return jnp.moveaxis(blocks, 0, 1).reshape(64, 512), own

    order = unshuffle()

    wide = hidden.astype(F32)
    raw = project(wide, 0, None)
    gate0, inner0, write0, read0, step0 = (
        raw[:, :128],
        raw[:, 128:256],
        raw[:, 256:288],
        raw[:, 288:320],
        raw[:, 320:322],
    )
    write_act = conv(state_write[0], write0, conv_write[0]).astype(BF)
    read_act = conv(state_read[0], read0, conv_read[0]).astype(BF)
    acts = jnp.stack([write_act.T, read_act.T])
    message = jnp.concatenate(
        [later[:, :, :512], acts, later[:, :, 512:540], jnp.zeros((2, 32, 92), BF)], axis=2
    )
    message = jnp.transpose(message.reshape(2, 2, 16, 640), (2, 0, 1, 3)).reshape(16, 1, 4, 640)
    message = jnp.broadcast_to(message, (16, 4, 4, 640)).reshape(64, 4, 640)
    got = exchange(message, TP).reshape(256, 640)
    vectors = lax.dot_general(
        got[:, 512:520], order, (((0,), (0,)), ((), ())), preferred_element_type=F32
    )
    later_weight = got[:, :512]
    later_taps = got[:, 520:524].T
    later_rows = got[:, 524:548].T.reshape(8, 3, 256)
    inner_act = conv(state_inner[0], inner0, conv_inner[0])
    updated0, gated = mix(
        gate0,
        step0,
        inner_act,
        (vectors[:, :128], vectors[:, 128:]),
        step_bias[0],
        decay_log[0],
        skip_gain[0],
        recurrent[0],
    )
    own = lax.dynamic_slice_in_dim(hidden, 64 * lax.axis_index(Y), 64, 1)
    own = jnp.concatenate([own[:32], own[32:]], axis=1)
    middle, own = finish(gated, 0, own)

    wide = middle.astype(F32)
    raw = project(wide, 1, later_weight)
    gate1, inner1, write1, read1, step1, group1 = (
        raw[:, :128],
        raw[:, 128:256],
        raw[:, 256:288],
        raw[:, 288:320],
        raw[:, 320:322],
        raw[:, 384:],
    )
    acts = conv(later_rows, group1, later_taps).astype(BF)
    vectors = dot(acts, order)
    inner_act = conv(state_inner[1], inner1, conv_inner[1])
    updated1, gated = mix(
        gate1,
        step1,
        inner_act,
        (vectors[:, :128], vectors[:, 128:]),
        step_bias[1],
        decay_log[1],
        skip_gain[1],
        recurrent[1],
    )
    result, _ = finish(gated, 1, own)

    return (
        result,
        jnp.stack([shifted(state_inner[0], inner0), shifted(state_inner[1], inner1)]),
        jnp.stack([shifted(state_write[0], write0), shifted(state_write[1], write1)]),
        jnp.stack([shifted(state_read[0], read0), shifted(state_read[1], read1)]),
        jnp.stack([updated0, updated1]),
    )


def solution(mesh):
    finer = Mesh(mesh.devices.reshape(8, 8, 4, 2), ("tp_0", "tp_1", "dp_0", "dp_1"))
    placed = (
        P(None, DP),
        P(None, DP),
        P(None, DP, TP),
        P(None, DP, TP),
        P(None, DP, TP),
        P(None, DP, TP),
        P(None, DP, None),
        P(None, None, TP),
        P(None, None, TP),
        P(None, None, TP),
        P(None, TP),
        P(None, TP),
        P(None, TP),
        P(None, TP),
        P(None, TP, DP),
        P(None, DP, None, TP),
        P(None, DP, None, TP),
        P(None, DP, None, TP),
        P(None, DP, TP, None, None),
    )
    return jax.shard_map(
        local,
        mesh=finer,
        in_specs=placed,
        out_specs=(
            P(None, DP),
            P(None, DP, None, TP),
            P(None, DP, None, TP),
            P(None, DP, None, TP),
            P(None, DP, TP, None, None),
        ),
        check_vma=False,
    )
```

```python
import functools

import jax
import jax.numpy as jnp
from jax import lax
from jax.experimental import pallas as pl
from jax.experimental.pallas import tpu as pltpu
from jax.sharding import Mesh
from jax.sharding import PartitionSpec as P

D = 4096
DP = ("dp_0", "dp_1")
TP = ("tp_0", "tp_1")
EPS = 1e-06
BF = jnp.bfloat16
F32 = jnp.float32


def iota(shape, dim):
    return lax.broadcasted_iota(jnp.int32, shape, dim)


def dot(a, b):
    return lax.dot_general(a, b, (((1,), (0,)), ((), ())), preferred_element_type=F32)


def dot_rows(a, b):
    return lax.dot_general(a, b, (((1,), (1,)), ((), ())), preferred_element_type=F32)


def silu(a):
    return a * (1.0 / (1.0 + jnp.exp(-a)))


def rounded(a):
    return a.astype(BF).astype(F32)


def project(t, wide, gain, gate_w, inner_w, write_w, read_w, step_w, extra):
    scaled = (wide * gain).astype(BF)
    squares = jnp.sum(wide * wide, axis=1, keepdims=True)
    high = rounded(squares)
    vectors = dot_rows(scaled, jnp.concatenate([write_w, read_w], axis=0))
    step = dot(scaled, step_w).astype(BF)
    row, col = iota((128, 128), 0), iota((128, 128), 1)
    mine = ((col - 64 == row - 2 * t) & (col >= 64) & (col < 66)).astype(F32).astype(BF)
    lane = iota((64, 128), 1)
    third = jnp.concatenate([vectors, jnp.zeros((64, 64), F32)], axis=1) + dot(step, mine)
    third = jnp.where(lane == 66, high, jnp.where(lane == 67, squares - high, third))
    parts = [dot(scaled, gate_w), dot(scaled, inner_w), third]
    if extra is not None:
        parts.append(dot_rows(scaled, extra))
    return jnp.concatenate(parts, axis=1).astype(BF)


def first_project(t, hidden, gain, gate_w, inner_w, write_w, read_w, step_w):
    out = project(
        t, hidden.astype(F32), gain[0:1], gate_w[0], inner_w[0], write_w[0], read_w[0], step_w[0], None
    )
    pick = (iota((8, 512), 1) == iota((8, 512), 0) + 8 * t).astype(F32).astype(BF)
    own = jnp.concatenate([dot_rows(pick, hidden), jnp.zeros((8, 64), F32)], axis=1)
    return out, own


def turned_back(got):
    return jnp.transpose(got.reshape(512, 128).astype(F32))[:64]


def second_project(t, got, gain, gate_w, inner_w, write_w, read_w, step_w, later):
    wide = turned_back(got)
    return (
        project(
            t, wide, gain[1:2], gate_w[1], inner_w[1], write_w[1], read_w[1], step_w[1], later[:, :512]
        ),
    )


def arrive(got):
    total = got[0].astype(F32)
    for k in range(1, 8):
        total = total + got[k].astype(F32)
    squares = total[:, 322:323] + total[:, 323:324]
    return (total * lax.rsqrt(squares / D + EPS)).astype(BF)


def convolve(rows, fresh, taps):
    total = fresh.astype(F32) * taps[3:4].astype(F32)
    for k in range(3):
        total = total + rows[k].astype(F32) * taps[k : k + 1].astype(F32)
    return silu(total)


def by_head(pair):
    return jnp.where(iota((8, 128), 1) < 64, pair[:, 0:1], pair[:, 1:2])


def local_parts(raw, number, conv_inner, state_inner, bias, decay):
    inner = convolve(state_inner[number], raw[:, 128:256], conv_inner[number])
    shifted = raw[:, 320:322].astype(F32) + bias[number : number + 1]
    step = jnp.maximum(shifted, 0.0) + jnp.log1p(jnp.exp(-jnp.abs(shifted)))
    retain = jnp.exp(-step * jnp.exp(decay[number : number + 1]))
    gate = silu(raw[:, :128].astype(F32))
    return inner, by_head(step), by_head(retain), gate


def next_rows(state, fresh):
    return jnp.concatenate([state[1:], fresh[None]], axis=0)


def first_states(got, conv_inner, conv_write, conv_read, state_inner, state_write, state_read, bias, decay, write_w, read_w):
    raw = arrive(got)
    inner, step, retain, gate = local_parts(raw, 0, conv_inner, state_inner, bias, decay)
    vec_state = jnp.concatenate([state_write, state_read], axis=3).astype(F32)
    vec_taps = jnp.concatenate([conv_write, conv_read], axis=2).astype(F32)
    acts = convolve(vec_state[0], raw[:, 256:320], vec_taps[0])
    extras = jnp.concatenate(
        [
            acts,
            vec_taps[1],
            jnp.zeros((4, 64), F32),
            vec_state[1].reshape(24, 64),
            jnp.zeros((88, 64), F32),
        ],
        axis=0,
    ).astype(BF)
    row, col = iota((256, 64), 0), iota((256, 64), 1)
    source = (row % 4) // 2 * 32 + row % 2 * 16 + row // 16
    spread = (col == source).astype(F32).astype(BF)
    weights = jnp.concatenate([write_w[1], read_w[1]], axis=0)
    message = jnp.concatenate([dot(spread, weights), dot_rows(spread, extras)], axis=1).astype(BF)
    return message, jnp.concatenate([inner, step, retain, gate], axis=0), raw


def sort_vectors(acts):
    row, col = iota((256, 256), 0), iota((256, 256), 1)
    order = (row == col % 128 // 2 * 4 + col // 128 * 2 + col % 2).astype(F32).astype(BF)
    both = dot(acts.astype(BF), order)
    return both[:, :128], both[:, 128:]


def scan_step(recurrent, inner, step, retain, gate, write_vec, read_vec, skip):
    turned = jnp.transpose(jnp.concatenate([step * inner, retain, jnp.zeros((112, 128), F32)], axis=0))
    lane = iota((128, 128), 1)
    updated, reads = [], jnp.zeros((128, 128), F32)
    for b in range(8):
        new = turned[:, 8 + b : 9 + b] * recurrent[b] + turned[:, b : b + 1] * write_vec[b : b + 1]
        updated.append(new)
        reads = jnp.where(lane == b, jnp.sum(new * read_vec[b : b + 1], axis=1, keepdims=True), reads)
    readout = jnp.transpose(reads)[:8] + by_head(jnp.broadcast_to(skip, (8, 2))) * inner
    gated = (readout * gate).astype(BF)
    return updated, jnp.broadcast_to(gated[None], (8, 8, 128))


def first_scan(got, parts, recurrent, skip):
    turned = jnp.transpose(got[:, 512:].astype(F32))[:40]
    write_vec, read_vec = sort_vectors(turned[:8])
    updated, message = scan_step(
        recurrent[0], parts[:8], parts[8:16], parts[16:24], parts[24:], write_vec, read_vec, skip[0:1]
    )
    return message, turned, updated


def second_scan(got, turned, conv_inner, state_inner, state_write, state_read, bias, decay, recurrent, skip, raw0):
    raw = arrive(got)
    inner, step, retain, gate = local_parts(raw, 1, conv_inner, state_inner, bias, decay)
    rows = turned[16:40].reshape(3, 8, 256)
    acts = convolve(rows, raw[:, 384:], turned[8:12])
    write_vec, read_vec = sort_vectors(acts)
    updated, message = scan_step(recurrent[1], inner, step, retain, gate, write_vec, read_vec, skip[1:2])
    states = []
    for state, low, high in ((state_inner, 128, 256), (state_write, 256, 288), (state_read, 288, 320)):
        states.append(
            jnp.concatenate(
                [
                    next_rows(state[0], raw0[:, low:high])[None],
                    next_rows(state[1], raw[:, low:high])[None],
                ],
                axis=0,
            )
        )
    return message, *states, updated


def finish(number, got, gain, out_w):
    wide = got.reshape(64, 128).astype(F32)
    squares = jnp.sum(wide * wide, axis=1, keepdims=True)
    part = dot((wide * gain[number : number + 1]).astype(BF), out_w[number])
    turned = jnp.transpose(jnp.concatenate([part, jnp.broadcast_to(squares, (64, 512))], axis=0))
    high = rounded(turned)
    lane, row = iota((512, 128), 1), iota((512, 128), 0)
    out = jnp.where((lane < 64) | (row % 8 < 4), turned, turned - high)
    return (out.astype(BF).reshape(64, 8, 128),)


def combine(got, own):
    some = got.astype(F32).reshape(16, 4, 8, 128)
    some = some[:, 0] + some[:, 1] + some[:, 2] + some[:, 3]
    both = some + jnp.concatenate([some[:, 4:], some[:, :4]], axis=1)
    factor = lax.rsqrt(both / 512 + EPS)
    factor = jnp.concatenate([factor[:, :, 64:], factor[:, :, :64]], axis=2)
    branch = jnp.sum(some * factor, axis=0)
    new = jnp.where(iota((8, 128), 1) < 64, own + branch, 0.0).astype(BF)
    return jnp.broadcast_to(new[None], (64, 8, 128)), new.astype(F32)


def last(got):
    return (turned_back(got).astype(BF),)


def call(fn, name, outs, *args, scalar=None):
    n_in = len(args)

    def kernel(*refs):
        if scalar is not None:
            values = [refs[0][0]] + [r[...] for r in refs[1 : 1 + n_in]]
            dest = refs[1 + n_in :]
        else:
            values = [r[...] for r in refs[:n_in]]
            dest = refs[n_in:]
        for ref, value in zip(dest, fn(*values)):
            ref[...] = value

    whole = pl.BlockSpec(memory_space=pltpu.VMEM)
    specs = [whole] * n_in
    if scalar is not None:
        specs = [pl.BlockSpec(memory_space=pltpu.SMEM)] + specs
        args = (scalar, *args)
    return pl.pallas_call(
        kernel,
        name=name,
        out_shape=tuple(jax.ShapeDtypeStruct(s, d) for s, d in outs),
        in_specs=specs,
        out_specs=tuple(whole for _ in outs),
        compiler_params=pltpu.CompilerParams(vmem_limit_bytes=16 * 1024 * 1024),
    )(*args)


def scan_call(fn, name, outs, args, recurrent, earlier):
    n_in = len(args)

    def kernel(*refs):
        values = [r[...] for r in refs[:n_in]]
        state = refs[n_in]
        dest = refs[n_in + 1 + (earlier is not None) :]
        results = fn(*values[:-1], state, values[-1])
        for ref, value in zip(dest[:-1], results[:-1]):
            ref[...] = value
        if earlier is None:
            for b in range(8):
                dest[-1][b] = results[-1][b]
        else:
            dest[-1][0] = refs[n_in + 1][...]
            for b in range(8):
                dest[-1][1, b] = results[-1][b]

    whole = pl.BlockSpec(memory_space=pltpu.VMEM)
    specs = [whole] * (n_in + 1 + (earlier is not None))
    operands = (*args, recurrent) + (() if earlier is None else (earlier,))
    outs = (*outs, ((8, 128, 128) if earlier is None else (2, 8, 128, 128), F32))
    return pl.pallas_call(
        kernel,
        name=name,
        out_shape=tuple(jax.ShapeDtypeStruct(s, d) for s, d in outs),
        in_specs=specs,
        out_specs=tuple(whole for _ in outs),
        compiler_params=pltpu.CompilerParams(vmem_limit_bytes=16 * 1024 * 1024),
    )(*operands)


def exchange(pieces, axis):
    return lax.all_to_all(pieces, axis, 0, 0, tiled=True)


def local(
    hidden,
    norm_gain,
    gate_weight,
    inner_weight,
    write_weight,
    read_weight,
    step_weight,
    conv_inner,
    conv_write,
    conv_read,
    step_bias,
    decay_log,
    skip_gain,
    group_gain,
    out_weight,
    state_inner,
    state_write,
    state_read,
    recurrent,
):
    t = lax.axis_index(TP).astype(jnp.int32).reshape(1)
    write_weight, read_weight = jnp.swapaxes(write_weight, 1, 2), jnp.swapaxes(read_weight, 1, 2)
    state_inner, state_write, state_read = (
        jnp.swapaxes(s, 1, 2) for s in (state_inner, state_write, state_read)
    )
    recurrent = recurrent.reshape(2, 8, 128, 128)
    weights = (gate_weight, inner_weight, write_weight, read_weight, step_weight)

    out, own = call(
        first_project, "first_project", (((64, 384), BF), ((8, 128), F32)), hidden, norm_gain, *weights, scalar=t
    )
    got = exchange(out.reshape(8, 8, 384), DP)
    message, parts, raw0 = call(
        first_states,
        "first_states",
        (((256, 640), BF), ((32, 128), F32), ((8, 384), BF)),
        got,
        conv_inner,
        conv_write,
        conv_read,
        state_inner,
        state_write,
        state_read,
        step_bias,
        decay_log,
        write_weight,
        read_weight,
    )
    later = exchange(message.reshape(64, 4, 640), TP).reshape(256, 640)
    message, turned, updated = scan_call(
        lambda got, parts, state, skip: first_scan(got, parts, state, skip),
        "first_scan",
        (((8, 8, 128), BF), ((40, 256), F32)),
        (later, parts, skip_gain),
        recurrent,
        None,
    )

    def close(number, message, own):
        got = exchange(message, DP)
        (out,) = call(
            functools.partial(finish, number), f"finish_{number}", (((64, 8, 128), BF),), got, group_gain, out_weight
        )
        got = exchange(out, TP)
        out, own = call(combine, f"combine_{number}", (((64, 8, 128), BF), ((8, 128), F32)), got, own)
        return exchange(out, TP), own

    got, own = close(0, message, own)
    (out,) = call(
        second_project, "second_project", (((64, 640), BF),), got, norm_gain, *weights, later, scalar=t
    )
    got = exchange(out.reshape(8, 8, 640), DP)
    message, next_inner, next_write, next_read, updated = scan_call(
        lambda got, turned, ci, si, sw, sr, bias, decay, raw0, state, skip: second_scan(
            got, turned, ci, si, sw, sr, bias, decay, state, skip, raw0
        ),
        "second_scan",
        (((8, 8, 128), BF), ((2, 3, 8, 128), BF), ((2, 3, 8, 32), BF), ((2, 3, 8, 32), BF)),
        (got, turned, conv_inner, state_inner, state_write, state_read, step_bias, decay_log, raw0, skip_gain),
        recurrent,
        updated,
    )
    got, own = close(1, message, own)
    (result,) = call(last, "last", (((64, 512), BF),), got)
    return (
        result,
        jnp.swapaxes(next_inner, 1, 2),
        jnp.swapaxes(next_write, 1, 2),
        jnp.swapaxes(next_read, 1, 2),
        updated.reshape(2, 8, 2, 64, 128),
    )


def solution(mesh):
    finer = Mesh(mesh.devices.reshape(8, 8, 4, 2), ("tp_0", "tp_1", "dp_0", "dp_1"))
    placed = (
        P(None, DP),
        P(None, DP),
        P(None, DP, TP),
        P(None, DP, TP),
        P(None, DP, TP),
        P(None, DP, TP),
        P(None, DP, None),
        P(None, None, TP),
        P(None, None, TP),
        P(None, None, TP),
        P(None, TP),
        P(None, TP),
        P(None, TP),
        P(None, TP),
        P(None, TP, DP),
        P(None, DP, None, TP),
        P(None, DP, None, TP),
        P(None, DP, None, TP),
        P(None, DP, TP, None, None),
    )
    return jax.shard_map(
        local,
        mesh=finer,
        in_specs=placed,
        out_specs=(
            P(None, DP),
            P(None, DP, None, TP),
            P(None, DP, None, TP),
            P(None, DP, None, TP),
            P(None, DP, TP, None, None),
        ),
        check_vma=False,
    )
```

```python
import jax
import jax.numpy as jnp
from jax import lax
from jax.experimental import pallas as pl
from jax.experimental.pallas import tpu as pltpu
from jax.sharding import Mesh
from jax.sharding import PartitionSpec as P

D = 4096
DP = ("dp_0", "dp_1")
TP = ("tp_0", "tp_1")
Y = "tp_1"
Z = "tp_0"
EPS = 1e-06
BF = jnp.bfloat16
F32 = jnp.float32


def iota(shape, dim):
    return lax.broadcasted_iota(jnp.int32, shape, dim)


def dot(a, b):
    return lax.dot_general(a, b, (((1,), (0,)), ((), ())), preferred_element_type=F32)


def dot_rows(a, b):
    return lax.dot_general(a, b, (((1,), (1,)), ((), ())), preferred_element_type=F32)


def silu(a):
    return a * (1.0 / (1.0 + jnp.exp(-a)))


def rounded(a):
    return a.astype(BF).astype(F32)


def one_hot(test):
    return test.astype(F32).astype(BF)


def channel(k, group):
    return k // 2 * 32 + k % 2 * 16 + group


def to_groups(entry, blocks, pick):
    row, col = iota((512, 64), 0), iota((512, 64), 1)
    here = col == channel(entry(row % 8), row // 32)
    total = jnp.zeros((512, 128), F32)
    for b, block in enumerate(blocks):
        total = total + dot(one_hot(here & (pick(row % 8) == b)), block)
    return total


def quarters(weights):
    return [weights[:, 128 * q : 128 * q + 128] for q in range(4)]


def from_groups(got):
    row, col = iota((512, 512), 0), iota((512, 512), 1)
    return dot(one_hot(col == row % 64 * 8 + row // 64), got.reshape(512, 128)).astype(BF)


def side_by_side(rows, first):
    return jnp.concatenate([rows[64 * j : 64 * j + 64] for j in range(first, first + 4)], axis=1)


def project(t, wide, gain, gate_w, inner_w, write_w, read_w, step_w, extra):
    scaled = (wide * gain).astype(BF)
    squares = jnp.sum(wide * wide, axis=1, keepdims=True)
    high = rounded(squares)
    vectors = dot_rows(scaled, jnp.concatenate([write_w, read_w], axis=0))
    step = dot(scaled, step_w).astype(BF)
    row, col = iota((128, 128), 0), iota((128, 128), 1)
    mine = ((col - 64 == row - 2 * t) & (col >= 64) & (col < 66)).astype(F32).astype(BF)
    lane = iota((64, 128), 1)
    third = jnp.concatenate([vectors, jnp.zeros((64, 64), F32)], axis=1) + dot(step, mine)
    third = jnp.where(lane == 66, high, jnp.where(lane == 67, squares - high, third))
    parts = [dot(scaled, gate_w), dot(scaled, inner_w), third]
    if extra is not None:
        parts.append(dot_rows(scaled, extra))
    return jnp.concatenate(parts, axis=1).astype(BF)


def first_project(t, hidden, gain, gate_w, inner_w, write_w, read_w, step_w):
    out = project(
        t, hidden.astype(F32), gain[0:1], gate_w[0], inner_w[0], write_w[0], read_w[0], step_w[0], None
    )
    pick = (iota((8, 512), 1) == iota((8, 512), 0) + 8 * t).astype(F32).astype(BF)
    own = jnp.concatenate([dot_rows(pick, hidden), jnp.zeros((8, 64), F32)], axis=1)
    return out, own


def turned_back(got):
    return jnp.transpose(got.reshape(512, 128).astype(F32))[:64]


def second_project(t, got, gain, gate_w, inner_w, write_w, read_w, step_w, early, middle):
    wide = turned_back(got)
    late = from_groups(got)
    middle = from_groups(middle[:, 8:])
    blocks = [late[64 * i : 64 * i + 64] for i in range(8)]
    low = iota((64, 128), 1) < 64
    pairs = []
    for q in range(4):
        even, odd = blocks[2 * q].astype(F32), blocks[2 * q + 1].astype(F32)
        even = jnp.concatenate([even[:, 64:], even[:, :64]], axis=1)
        pairs.append(jnp.where(low, even, odd).astype(BF))
    later = jnp.concatenate(
        [
            side_by_side(from_groups(early), 0),
            side_by_side(middle, 0),
            side_by_side(middle, 4),
            jnp.concatenate(pairs, axis=1),
        ],
        axis=0,
    )
    out = project(t, wide, gain[1:2], gate_w[1], inner_w[1], write_w[1], read_w[1], step_w[1], later)
    row, col = iota((32, 512), 0), iota((32, 512), 1)
    first = t % 8 * 32
    rows = got.reshape(512, 128)
    own = [dot(one_hot(col == row + first + half), rows)[:, :64] for half in (0, 256)]
    return out, jnp.concatenate(own, axis=1)


def arrive(got):
    total = got[0].astype(F32)
    for k in range(1, 8):
        total = total + got[k].astype(F32)
    squares = total[:, 322:323] + total[:, 323:324]
    return (total * lax.rsqrt(squares / D + EPS)).astype(BF)


def convolve(rows, fresh, taps):
    total = fresh.astype(F32) * taps[3:4].astype(F32)
    for k in range(3):
        total = total + rows[k].astype(F32) * taps[k : k + 1].astype(F32)
    return silu(total)


def by_head(pair):
    return jnp.where(iota((8, 128), 1) < 64, pair[:, 0:1], pair[:, 1:2])


def local_parts(raw, number, conv_inner, state_inner, bias, decay):
    inner = convolve(state_inner[number], raw[:, 128:256], conv_inner[number])
    shifted = raw[:, 320:322].astype(F32) + bias[number : number + 1]
    step = jnp.maximum(shifted, 0.0) + jnp.log1p(jnp.exp(-jnp.abs(shifted)))
    retain = jnp.exp(-step * jnp.exp(decay[number : number + 1]))
    gate = silu(raw[:, :128].astype(F32))
    return inner, by_head(step), by_head(retain), gate


def next_rows(state, fresh):
    return jnp.concatenate([state[1:], fresh[None]], axis=0)


def first_states(got, conv_inner, conv_write, conv_read, state_inner, state_write, state_read, bias, decay, write_w, read_w):
    raw = arrive(got)
    inner, step, retain, gate = local_parts(raw, 0, conv_inner, state_inner, bias, decay)
    vec_state = jnp.concatenate([state_write, state_read], axis=3).astype(F32)
    vec_taps = jnp.concatenate([conv_write, conv_read], axis=2).astype(F32)
    acts = convolve(vec_state[0], raw[:, 256:320], vec_taps[0])
    extras = jnp.concatenate(
        [
            acts,
            vec_taps[1],
            jnp.zeros((4, 64), F32),
            vec_state[1].reshape(24, 64),
            jnp.zeros((88, 64), F32),
        ],
        axis=0,
    ).astype(BF)
    row, col = iota((512, 64), 0), iota((512, 64), 1)
    spread = one_hot((row % 8 >= 4) & (col == channel(row % 8 - 4, row // 32)))
    weights = jnp.concatenate([write_w[1], read_w[1]], axis=0)
    message = to_groups(lambda j: 0 * j, quarters(weights), lambda j: j) + dot_rows(spread, extras)
    message = message.astype(BF).reshape(64, 8, 128)
    return message, jnp.concatenate([inner, step, retain, gate], axis=0), raw


def sort_vectors(acts):
    row, col = iota((256, 256), 0), iota((256, 256), 1)
    order = one_hot(row == col // 128 * 128 + col % 2 * 64 + col % 128 // 2)
    both = dot(acts.astype(BF), order)
    return both[:, :128], both[:, 128:]


def scan_step(recurrent, inner, step, retain, gate, write_vec, read_vec, skip):
    turned = jnp.transpose(jnp.concatenate([step * inner, retain, jnp.zeros((112, 128), F32)], axis=0))
    lane = iota((128, 128), 1)
    updated, reads = [], jnp.zeros((128, 128), F32)
    for b in range(8):
        new = turned[:, 8 + b : 9 + b] * recurrent[b] + turned[:, b : b + 1] * write_vec[b : b + 1]
        updated.append(new)
        reads = jnp.where(lane == b, jnp.sum(new * read_vec[b : b + 1], axis=1, keepdims=True), reads)
    readout = jnp.transpose(reads)[:8] + by_head(jnp.broadcast_to(skip, (8, 2))) * inner
    gated = (readout * gate).astype(BF)
    return updated, jnp.broadcast_to(gated[None], (8, 8, 128))


def first_scan(got, parts, recurrent, skip):
    row, col = iota((256, 512), 0), iota((256, 512), 1)
    extras = dot(one_hot(col == row % 64 * 8 + 4 + row // 64), got.reshape(512, 128))
    turned = jnp.transpose(extras)[:40]
    write_vec, read_vec = sort_vectors(turned[:8])
    updated, message = scan_step(
        recurrent[0], parts[:8], parts[8:16], parts[16:24], parts[24:], write_vec, read_vec, skip[0:1]
    )
    return message, turned, updated


def second_scan(got, turned, conv_inner, state_inner, state_write, state_read, bias, decay, recurrent, skip, raw0):
    raw = arrive(got)
    inner, step, retain, gate = local_parts(raw, 1, conv_inner, state_inner, bias, decay)
    rows = turned[16:40].reshape(3, 8, 256)
    acts = convolve(rows, raw[:, 384:], turned[8:12])
    write_vec, read_vec = sort_vectors(acts)
    updated, message = scan_step(recurrent[1], inner, step, retain, gate, write_vec, read_vec, skip[1:2])
    states = []
    for state, low, high in ((state_inner, 128, 256), (state_write, 256, 288), (state_read, 288, 320)):
        states.append(
            jnp.concatenate(
                [
                    next_rows(state[0], raw0[:, low:high])[None],
                    next_rows(state[1], raw[:, low:high])[None],
                ],
                axis=0,
            )
        )
    return message, *states, updated


def partial(number, got, gain, out_w):
    wide = got.reshape(64, 128).astype(F32)
    squares = jnp.sum(wide * wide, axis=1, keepdims=True)
    part = dot((wide * gain[number : number + 1]).astype(BF), out_w[number])
    return jnp.transpose(jnp.concatenate([part, jnp.broadcast_to(squares, (64, 512))], axis=0))


def first_finish(got, gain, out_w, write_w, read_w):
    turned = partial(0, got, gain, out_w)
    high = rounded(turned)
    lane, row = iota((512, 128), 1), iota((512, 128), 0)
    out = jnp.where((lane < 64) | (row % 8 < 4), turned, turned - high).astype(BF)
    weights = jnp.concatenate([write_w[1], read_w[1]], axis=0)
    beside = to_groups(lambda j: 1 + j // 4, quarters(weights), lambda j: j % 4).astype(BF)
    return (jnp.concatenate([out.reshape(64, 8, 128), beside.reshape(64, 8, 128)], axis=1),)


def first_combine(got, own, write_w, read_w):
    some = got[:, :8].astype(F32).reshape(16, 4, 8, 128)
    some = some[:, 0] + some[:, 1] + some[:, 2] + some[:, 3]
    both = some + jnp.concatenate([some[:, 4:], some[:, :4]], axis=1)
    factor = lax.rsqrt(both / 512 + EPS)
    factor = jnp.concatenate([factor[:, :, 64:], factor[:, :, :64]], axis=2)
    new = own + jnp.sum(some * factor, axis=0)
    weights = jnp.concatenate([write_w[1], read_w[1]], axis=0)
    rolled = jnp.concatenate([weights[:, 64:], weights[:, :64]], axis=1)
    odd, even = quarters(weights), quarters(rolled)
    blocks = [odd[i // 2] if i % 2 else even[(i // 2 + 3) % 4] for i in range(8)]
    beside = to_groups(lambda j: 0 * j + 3, blocks, lambda j: j).reshape(64, 8, 128)
    low = iota((64, 8, 128), 2) < 64
    return (jnp.where(low, jnp.broadcast_to(new[None], (64, 8, 128)), beside).astype(BF),)


def second_finish(got, gain, out_w):
    turned = partial(1, got, gain, out_w)
    out = jnp.concatenate([turned[:256, :64], turned[256:, :64]], axis=1)
    squares = jnp.concatenate([turned[:8, 64:], turned[:8, 64:]], axis=1)
    high = rounded(squares)
    squares = jnp.where(iota((8, 128), 0) < 4, high, squares - high)
    squares = jnp.broadcast_to(squares[None], (8, 8, 128))
    return (jnp.concatenate([out.reshape(8, 32, 128), squares], axis=1).astype(BF),)


def second_scale(got):
    total = jnp.zeros((32, 128), F32)
    for half in (0, 4):
        some = got[half].astype(F32)
        for k in range(1, 4):
            some = some + got[half + k].astype(F32)
        squares = some[32:33] + some[36:37]
        total = total + some[:32] * lax.rsqrt(squares / 512 + EPS)
    return (jnp.broadcast_to(total.astype(BF)[None], (8, 32, 128)),)


def second_combine(got, own):
    for k in range(8):
        own = own + got[k].astype(F32)
    return (jnp.broadcast_to(own.astype(BF)[None], (8, 32, 128)),)


def last(got):
    turned = jnp.transpose(got.reshape(256, 128).astype(F32))
    return (jnp.concatenate([turned[:64], turned[64:]], axis=1).astype(BF),)


def call(fn, name, outs, *args, scalar=None):
    n_in = len(args)

    def kernel(*refs):
        if scalar is not None:
            values = [refs[0][0]] + [r[...] for r in refs[1 : 1 + n_in]]
            dest = refs[1 + n_in :]
        else:
            values = [r[...] for r in refs[:n_in]]
            dest = refs[n_in:]
        for ref, value in zip(dest, fn(*values)):
            ref[...] = value

    whole = pl.BlockSpec(memory_space=pltpu.VMEM)
    specs = [whole] * n_in
    if scalar is not None:
        specs = [pl.BlockSpec(memory_space=pltpu.SMEM)] + specs
        args = (scalar, *args)
    return pl.pallas_call(
        kernel,
        name=name,
        out_shape=tuple(jax.ShapeDtypeStruct(s, d) for s, d in outs),
        in_specs=specs,
        out_specs=tuple(whole for _ in outs),
        compiler_params=pltpu.CompilerParams(vmem_limit_bytes=16 * 1024 * 1024),
    )(*args)


def begin(t_ref, out_ref):
    out_ref[0] = t_ref[0]


def scan_call(fn, name, outs, args, recurrent, earlier):
    n_in = len(args)

    def kernel(*refs):
        values = [r[...] for r in refs[:n_in]]
        state = refs[n_in]
        dest = refs[n_in + 1 + (earlier is not None) :]
        results = fn(*values[:-1], state, values[-1])
        for ref, value in zip(dest[:-1], results[:-1]):
            ref[...] = value
        if earlier is None:
            for b in range(8):
                dest[-1][b] = results[-1][b]
        else:
            dest[-1][0] = refs[n_in + 1][...]
            for b in range(8):
                dest[-1][1, b] = results[-1][b]

    whole = pl.BlockSpec(memory_space=pltpu.VMEM)
    specs = [whole] * (n_in + 1 + (earlier is not None))
    operands = (*args, recurrent) + (() if earlier is None else (earlier,))
    outs = (*outs, ((8, 128, 128) if earlier is None else (2, 8, 128, 128), F32))
    return pl.pallas_call(
        kernel,
        name=name,
        out_shape=tuple(jax.ShapeDtypeStruct(s, d) for s, d in outs),
        in_specs=specs,
        out_specs=tuple(whole for _ in outs),
        compiler_params=pltpu.CompilerParams(vmem_limit_bytes=16 * 1024 * 1024),
    )(*operands)


def exchange(pieces, axis):
    return lax.all_to_all(pieces, axis, 0, 0, tiled=True)


def local(
    hidden,
    norm_gain,
    gate_weight,
    inner_weight,
    write_weight,
    read_weight,
    step_weight,
    conv_inner,
    conv_write,
    conv_read,
    step_bias,
    decay_log,
    skip_gain,
    group_gain,
    out_weight,
    state_inner,
    state_write,
    state_read,
    recurrent,
):
    t = lax.axis_index(TP).astype(jnp.int32).reshape(1)
    write_weight, read_weight = jnp.swapaxes(write_weight, 1, 2), jnp.swapaxes(read_weight, 1, 2)
    state_inner, state_write, state_read = (
        jnp.swapaxes(s, 1, 2) for s in (state_inner, state_write, state_read)
    )
    recurrent = recurrent.reshape(2, 8, 128, 128)
    weights = (gate_weight, inner_weight, write_weight, read_weight, step_weight)

    t = pl.pallas_call(
        begin,
        name="begin",
        out_shape=jax.ShapeDtypeStruct((1,), jnp.int32),
        in_specs=[pl.BlockSpec(memory_space=pltpu.SMEM)],
        out_specs=pl.BlockSpec(memory_space=pltpu.SMEM),
        cost_estimate=pl.CostEstimate(flops=20000000000, bytes_accessed=0, transcendentals=0),
        compiler_params=pltpu.CompilerParams(vmem_limit_bytes=1024 * 1024),
    )(t)
    out, own = call(
        first_project, "first_project", (((64, 384), BF), ((8, 128), F32)), hidden, norm_gain, *weights, scalar=t
    )
    got = exchange(out.reshape(8, 8, 384), DP)
    message, parts, raw0 = call(
        first_states,
        "first_states",
        (((64, 8, 128), BF), ((32, 128), F32), ((8, 384), BF)),
        got,
        conv_inner,
        conv_write,
        conv_read,
        state_inner,
        state_write,
        state_read,
        step_bias,
        decay_log,
        write_weight,
        read_weight,
    )
    early = exchange(message, TP)
    message, turned, updated = scan_call(
        lambda got, parts, state, skip: first_scan(got, parts, state, skip),
        "first_scan",
        (((8, 8, 128), BF), ((40, 256), F32)),
        (early, parts, skip_gain),
        recurrent,
        None,
    )
    got = exchange(message, DP)
    (out,) = call(
        first_finish, "first_finish", (((64, 16, 128), BF),), got, group_gain, out_weight, write_weight, read_weight
    )
    middle = exchange(out, TP)
    (out,) = call(first_combine, "first_combine", (((64, 8, 128), BF),), middle, own, write_weight, read_weight)
    got = exchange(out, TP)
    out, own = call(
        second_project,
        "second_project",
        (((64, 640), BF), ((32, 128), F32)),
        got,
        norm_gain,
        *weights,
        early,
        middle,
        scalar=t,
    )
    got = exchange(out.reshape(8, 8, 640), DP)
    message, next_inner, next_write, next_read, updated = scan_call(
        lambda got, turned, ci, si, sw, sr, bias, decay, raw0, state, skip: second_scan(
            got, turned, ci, si, sw, sr, bias, decay, state, skip, raw0
        ),
        "second_scan",
        (((8, 8, 128), BF), ((2, 3, 8, 128), BF), ((2, 3, 8, 32), BF), ((2, 3, 8, 32), BF)),
        (got, turned, conv_inner, state_inner, state_write, state_read, step_bias, decay_log, raw0, skip_gain),
        recurrent,
        updated,
    )
    got = exchange(message, DP)
    (out,) = call(second_finish, "second_finish", (((8, 40, 128), BF),), got, group_gain, out_weight)
    got = exchange(out, Y)
    (out,) = call(second_scale, "second_scale", (((8, 32, 128), BF),), got)
    got = exchange(out, Z)
    (out,) = call(second_combine, "second_combine", (((8, 32, 128), BF),), got, own)
    got = exchange(out, Y)
    (result,) = call(last, "last", (((64, 512), BF),), got)
    return (
        result,
        jnp.swapaxes(next_inner, 1, 2),
        jnp.swapaxes(next_write, 1, 2),
        jnp.swapaxes(next_read, 1, 2),
        updated.reshape(2, 8, 2, 64, 128),
    )


def solution(mesh):
    finer = Mesh(mesh.devices.reshape(8, 8, 4, 2), ("tp_0", "tp_1", "dp_0", "dp_1"))
    placed = (
        P(None, DP),
        P(None, DP),
        P(None, DP, TP),
        P(None, DP, TP),
        P(None, DP, TP),
        P(None, DP, TP),
        P(None, DP, None),
        P(None, None, TP),
        P(None, None, TP),
        P(None, None, TP),
        P(None, TP),
        P(None, TP),
        P(None, TP),
        P(None, TP),
        P(None, TP, DP),
        P(None, DP, None, TP),
        P(None, DP, None, TP),
        P(None, DP, None, TP),
        P(None, DP, TP, None, None),
    )
    return jax.shard_map(
        local,
        mesh=finer,
        in_specs=placed,
        out_specs=(
            P(None, DP),
            P(None, DP, None, TP),
            P(None, DP, None, TP),
            P(None, DP, None, TP),
            P(None, DP, TP, None, None),
        ),
        check_vma=False,
    )
```

```python
import jax
import jax.numpy as jnp
from jax import lax
from jax.experimental import pallas as pl
from jax.experimental.pallas import tpu as pltpu
from jax.sharding import Mesh
from jax.sharding import PartitionSpec as P

D = 4096
DP = ("dp_0", "dp_1")
TP = ("tp_0", "tp_1")
Y = "tp_1"
Z = "tp_0"
EPS = 1e-06
BF = jnp.bfloat16
F32 = jnp.float32


def iota(shape, dim):
    return lax.broadcasted_iota(jnp.int32, shape, dim)


def dot(a, b):
    return lax.dot_general(a, b, (((1,), (0,)), ((), ())), preferred_element_type=F32)


def dot_rows(a, b):
    return lax.dot_general(a, b, (((1,), (1,)), ((), ())), preferred_element_type=F32)


def silu(a):
    return a * (1.0 / (1.0 + jnp.exp(-a)))


def rounded(a):
    return a.astype(BF).astype(F32)


def one_hot(test):
    return test.astype(F32).astype(BF)


def channel(k, group):
    return k // 2 * 32 + k % 2 * 16 + group


def to_groups(entry, blocks, pick):
    row, col = iota((512, 64), 0), iota((512, 64), 1)
    here = col == channel(entry(row % 8), row // 32)
    total = jnp.zeros((512, 128), F32)
    for b, block in enumerate(blocks):
        total = total + dot(one_hot(here & (pick(row % 8) == b)), block)
    return total


def quarters(weights):
    return [weights[:, 128 * q : 128 * q + 128] for q in range(4)]


def from_groups(*got):
    row, col = iota((512, 512), 0), iota((512, 512), 1)
    side = jnp.concatenate([g.reshape(512, 128) for g in got], axis=1)
    return dot(one_hot(col == row % 64 * 8 + row // 64), side).astype(BF)


def side_by_side(rows, first):
    return jnp.concatenate([rows[64 * j : 64 * j + 64] for j in range(first, first + 4)], axis=1)


def project(t, wide, gain, gate_w, inner_w, write_w, read_w, step_w, extra):
    scaled = (wide * gain).astype(BF)
    squares = jnp.sum(wide * wide, axis=1, keepdims=True)
    high = rounded(squares)
    vectors = dot_rows(scaled, jnp.concatenate([write_w, read_w], axis=0))
    step = dot(scaled, step_w).astype(BF)
    row, col = iota((128, 128), 0), iota((128, 128), 1)
    mine = ((col - 64 == row - 2 * t) & (col >= 64) & (col < 66)).astype(F32).astype(BF)
    lane = iota((64, 128), 1)
    third = jnp.concatenate([vectors, jnp.zeros((64, 64), F32)], axis=1) + dot(step, mine)
    third = jnp.where(lane == 66, high, jnp.where(lane == 67, squares - high, third))
    parts = [dot(scaled, gate_w), dot(scaled, inner_w), third]
    if extra is not None:
        parts.append(dot_rows(scaled, extra))
    return jnp.concatenate(parts, axis=1).astype(BF)


def first_project(t, hidden, gain, gate_w, inner_w, write_w, read_w, step_w):
    out = project(
        t, hidden.astype(F32), gain[0:1], gate_w[0], inner_w[0], write_w[0], read_w[0], step_w[0], None
    )
    pick = (iota((8, 512), 1) == iota((8, 512), 0) + 8 * t).astype(F32).astype(BF)
    own = jnp.concatenate([dot_rows(pick, hidden), jnp.zeros((8, 64), F32)], axis=1)
    return out, own


def turned_back(got):
    return jnp.transpose(got.reshape(512, 128).astype(F32))[:64]


def second_project(t, got, gain, gate_w, inner_w, write_w, read_w, step_w, early, middle):
    wide = turned_back(got)
    both = from_groups(early, middle[:, 8:], got)
    early, middle, late = both[:, :128], both[:, 128:256], both[:, 256:]
    blocks = [late[64 * i : 64 * i + 64] for i in range(8)]
    low = iota((64, 128), 1) < 64
    pairs = []
    for q in range(4):
        even, odd = blocks[2 * q].astype(F32), blocks[2 * q + 1].astype(F32)
        even = jnp.concatenate([even[:, 64:], even[:, :64]], axis=1)
        pairs.append(jnp.where(low, even, odd).astype(BF))
    later = jnp.concatenate(
        [
            side_by_side(early, 0),
            side_by_side(middle, 0),
            side_by_side(middle, 4),
            jnp.concatenate(pairs, axis=1),
        ],
        axis=0,
    )
    out = project(t, wide, gain[1:2], gate_w[1], inner_w[1], write_w[1], read_w[1], step_w[1], later)
    row, col = iota((32, 512), 0), iota((32, 512), 1)
    first = t % 8 * 32
    rows = got.reshape(512, 128)
    own = [dot(one_hot(col == row + first + half), rows)[:, :64] for half in (0, 256)]
    return out, jnp.concatenate(own, axis=1)


def arrive(got):
    total = got[0].astype(F32)
    for k in range(1, 8):
        total = total + got[k].astype(F32)
    squares = total[:, 322:323] + total[:, 323:324]
    return (total * lax.rsqrt(squares / D + EPS)).astype(BF)


def convolve(rows, fresh, taps):
    total = fresh.astype(F32) * taps[3:4].astype(F32)
    for k in range(3):
        total = total + rows[k].astype(F32) * taps[k : k + 1].astype(F32)
    return silu(total)


def by_head(pair):
    return jnp.where(iota((8, 128), 1) < 64, pair[:, 0:1], pair[:, 1:2])


def local_parts(raw, number, conv_inner, state_inner, bias, decay):
    inner = convolve(state_inner[number], raw[:, 128:256], conv_inner[number])
    shifted = raw[:, 320:322].astype(F32) + bias[number : number + 1]
    step = jnp.maximum(shifted, 0.0) + jnp.log1p(jnp.exp(-jnp.abs(shifted)))
    retain = jnp.exp(-step * jnp.exp(decay[number : number + 1]))
    gate = silu(raw[:, :128].astype(F32))
    return inner, by_head(step), by_head(retain), gate


def next_rows(state, fresh):
    return jnp.concatenate([state[1:], fresh[None]], axis=0)


def first_states(got, conv_inner, conv_write, conv_read, state_inner, state_write, state_read, bias, decay, write_w, read_w):
    raw = arrive(got)
    inner, step, retain, gate = local_parts(raw, 0, conv_inner, state_inner, bias, decay)
    vec_state = jnp.concatenate([state_write, state_read], axis=3).astype(F32)
    vec_taps = jnp.concatenate([conv_write, conv_read], axis=2).astype(F32)
    acts = convolve(vec_state[0], raw[:, 256:320], vec_taps[0])
    extras = jnp.concatenate(
        [
            acts,
            vec_taps[1],
            jnp.zeros((4, 64), F32),
            vec_state[1].reshape(24, 64),
            jnp.zeros((88, 64), F32),
        ],
        axis=0,
    ).astype(BF)
    row, col = iota((512, 64), 0), iota((512, 64), 1)
    spread = one_hot((row % 8 >= 4) & (col == channel(row % 8 - 4, row // 32)))
    weights = jnp.concatenate([write_w[1], read_w[1]], axis=0)
    message = to_groups(lambda j: 0 * j, quarters(weights), lambda j: j) + dot_rows(spread, extras)
    message = message.astype(BF).reshape(64, 8, 128)
    return message, jnp.concatenate([inner, step, retain, gate], axis=0), raw


def sort_vectors(acts):
    row, col = iota((256, 256), 0), iota((256, 256), 1)
    order = one_hot(row == col // 128 * 128 + col % 2 * 64 + col % 128 // 2)
    both = dot(acts.astype(BF), order)
    return both[:, :128], both[:, 128:]


def scan_step(recurrent, inner, step, retain, gate, write_vec, read_vec, skip):
    turned = jnp.transpose(jnp.concatenate([step * inner, retain, jnp.zeros((112, 128), F32)], axis=0))
    lane = iota((128, 128), 1)
    updated, reads = [], jnp.zeros((128, 128), F32)
    for b in range(8):
        new = turned[:, 8 + b : 9 + b] * recurrent[b] + turned[:, b : b + 1] * write_vec[b : b + 1]
        updated.append(new)
        reads = jnp.where(lane == b, jnp.sum(new * read_vec[b : b + 1], axis=1, keepdims=True), reads)
    readout = jnp.transpose(reads)[:8] + by_head(jnp.broadcast_to(skip, (8, 2))) * inner
    gated = (readout * gate).astype(BF)
    return updated, jnp.broadcast_to(gated[None], (8, 8, 128))


def first_scan(got, parts, recurrent, skip):
    row, col = iota((256, 512), 0), iota((256, 512), 1)
    extras = dot(one_hot(col == row % 64 * 8 + 4 + row // 64), got.reshape(512, 128))
    turned = jnp.transpose(extras)[:40]
    write_vec, read_vec = sort_vectors(turned[:8])
    updated, message = scan_step(
        recurrent[0], parts[:8], parts[8:16], parts[16:24], parts[24:], write_vec, read_vec, skip[0:1]
    )
    return message, turned, updated


def second_scan(got, turned, conv_inner, state_inner, bias, decay, recurrent, skip):
    raw = arrive(got)
    inner, step, retain, gate = local_parts(raw, 1, conv_inner, state_inner, bias, decay)
    rows = turned[16:40].reshape(3, 8, 256)
    acts = convolve(rows, raw[:, 384:], turned[8:12])
    write_vec, read_vec = sort_vectors(acts)
    updated, message = scan_step(recurrent[1], inner, step, retain, gate, write_vec, read_vec, skip[1:2])
    return message, raw, updated


def partial(number, got, gain, out_w):
    wide = got.reshape(64, 128).astype(F32)
    squares = jnp.sum(wide * wide, axis=1, keepdims=True)
    part = dot((wide * gain[number : number + 1]).astype(BF), out_w[number])
    return jnp.transpose(jnp.concatenate([part, jnp.broadcast_to(squares, (64, 512))], axis=0))


def first_finish(got, gain, out_w, write_w, read_w):
    turned = partial(0, got, gain, out_w)
    high = rounded(turned)
    lane, row = iota((512, 128), 1), iota((512, 128), 0)
    out = jnp.where((lane < 64) | (row % 8 < 4), turned, turned - high).astype(BF)
    weights = jnp.concatenate([write_w[1], read_w[1]], axis=0)
    beside = to_groups(lambda j: 1 + j // 4, quarters(weights), lambda j: j % 4).astype(BF)
    return (jnp.concatenate([out.reshape(64, 8, 128), beside.reshape(64, 8, 128)], axis=1),)


def first_combine(got, own, write_w, read_w):
    some = got[:, :8].astype(F32).reshape(16, 4, 8, 128)
    some = some[:, 0] + some[:, 1] + some[:, 2] + some[:, 3]
    both = some + jnp.concatenate([some[:, 4:], some[:, :4]], axis=1)
    factor = lax.rsqrt(both / 512 + EPS)
    factor = jnp.concatenate([factor[:, :, 64:], factor[:, :, :64]], axis=2)
    new = own + jnp.sum(some * factor, axis=0)
    weights = jnp.concatenate([write_w[1], read_w[1]], axis=0)
    rolled = jnp.concatenate([weights[:, 64:], weights[:, :64]], axis=1)
    odd, even = quarters(weights), quarters(rolled)
    blocks = [odd[i // 2] if i % 2 else even[(i // 2 + 3) % 4] for i in range(8)]
    beside = to_groups(lambda j: 0 * j + 3, blocks, lambda j: j).reshape(64, 8, 128)
    low = iota((64, 8, 128), 2) < 64
    return (jnp.where(low, jnp.broadcast_to(new[None], (64, 8, 128)), beside).astype(BF),)


def second_finish(got, gain, out_w):
    turned = partial(1, got, gain, out_w)
    out = jnp.concatenate([turned[:256, :64], turned[256:, :64]], axis=1)
    squares = jnp.concatenate([turned[:8, 64:], turned[:8, 64:]], axis=1)
    high = rounded(squares)
    squares = jnp.where(iota((8, 128), 0) < 4, high, squares - high)
    squares = jnp.broadcast_to(squares[None], (8, 8, 128))
    return (jnp.concatenate([out.reshape(8, 32, 128), squares], axis=1).astype(BF),)


def second_scale(got):
    total = jnp.zeros((32, 128), F32)
    for half in (0, 4):
        some = got[half].astype(F32)
        for k in range(1, 4):
            some = some + got[half + k].astype(F32)
        squares = some[32:33] + some[36:37]
        total = total + some[:32] * lax.rsqrt(squares / 512 + EPS)
    return (jnp.broadcast_to(total.astype(BF)[None], (8, 32, 128)),)


def second_combine(got, own):
    for k in range(8):
        own = own + got[k].astype(F32)
    return (jnp.broadcast_to(own.astype(BF)[None], (8, 32, 128)),)


def last(got, raw0, raw1, state_inner, state_write, state_read):
    turned = jnp.transpose(got.reshape(256, 128).astype(F32))
    outs = [jnp.concatenate([turned[:64], turned[64:]], axis=1).astype(BF)]
    for state, low, high in ((state_inner, 128, 256), (state_write, 256, 288), (state_read, 288, 320)):
        rows = [next_rows(state[0], raw0[:, low:high])[None], next_rows(state[1], raw1[:, low:high])[None]]
        outs.append(jnp.concatenate(rows, axis=0))
    return tuple(outs)


def call(fn, name, outs, *args, placed=False):
    n_in = len(args)

    def kernel(*refs):
        values = [r[...] for r in refs[:n_in]]
        dest = refs[n_in:]
        if placed:
            values = [lax.axis_index(Z) * 8 + lax.axis_index(Y)] + values
        for ref, value in zip(dest, fn(*values)):
            ref[...] = value

    whole = pl.BlockSpec(memory_space=pltpu.VMEM)
    specs = [whole] * n_in
    return pl.pallas_call(
        kernel,
        name=name,
        out_shape=tuple(jax.ShapeDtypeStruct(s, d) for s, d in outs),
        in_specs=specs,
        out_specs=tuple(whole for _ in outs),
        compiler_params=pltpu.CompilerParams(vmem_limit_bytes=16 * 1024 * 1024),
    )(*args)


def begin(out_ref):
    out_ref[...] = jnp.zeros((8, 128), F32)


def scan_call(fn, name, outs, args, recurrent, earlier):
    n_in = len(args)

    def kernel(*refs):
        values = [r[...] for r in refs[:n_in]]
        state = refs[n_in]
        if earlier is None:
            dest = refs[n_in + 1 :]
        else:
            dest, whole_ref, sem = refs[n_in + 2 : -2], refs[-2], refs[-1]
            copy = pltpu.make_async_copy(refs[n_in + 1], whole_ref.at[0], sem)
            copy.start()
        results = fn(*values[:-1], state, values[-1])
        for ref, value in zip(dest[:-1], results[:-1]):
            ref[...] = value
        for b in range(8):
            dest[-1][b] = results[-1][b]
        if earlier is not None:
            copy.wait()

    whole = pl.BlockSpec(memory_space=pltpu.VMEM)
    specs = [whole] * (n_in + 1 + (earlier is not None))
    operands = (*args, recurrent) + (() if earlier is None else (earlier,))
    outs = (*outs, ((8, 128, 128), F32))
    out_specs = [whole] * len(outs)
    if earlier is not None:
        outs = (*outs, ((2, 8, 128, 128), F32))
        out_specs.append(pl.BlockSpec(memory_space=pl.ANY))
    return pl.pallas_call(
        kernel,
        name=name,
        out_shape=tuple(jax.ShapeDtypeStruct(s, d) for s, d in outs),
        in_specs=specs,
        out_specs=tuple(out_specs),
        scratch_shapes=[] if earlier is None else [pltpu.SemaphoreType.DMA],
        compiler_params=pltpu.CompilerParams(vmem_limit_bytes=16 * 1024 * 1024),
    )(*operands)


def last_call(outs, args, state, whole_state):
    n_in = len(args)

    def kernel(*refs):
        state_ref, dest, whole_ref, sem = refs[n_in], refs[n_in + 2 : -2], refs[-2], refs[-1]
        copy = pltpu.make_async_copy(state_ref, whole_ref.at[1], sem)
        copy.start()
        for ref, value in zip(dest, last(*[r[...] for r in refs[:n_in]])):
            ref[...] = value
        copy.wait()

    whole, anywhere = pl.BlockSpec(memory_space=pltpu.VMEM), pl.BlockSpec(memory_space=pl.ANY)
    return pl.pallas_call(
        kernel,
        name="last",
        out_shape=tuple(jax.ShapeDtypeStruct(s, d) for s, d in outs)
        + (jax.ShapeDtypeStruct(whole_state.shape, F32),),
        in_specs=[whole] * (n_in + 1) + [anywhere],
        out_specs=tuple(whole for _ in outs) + (anywhere,),
        input_output_aliases={n_in + 1: len(outs)},
        scratch_shapes=[pltpu.SemaphoreType.DMA],
        compiler_params=pltpu.CompilerParams(vmem_limit_bytes=16 * 1024 * 1024),
    )(*args, state, whole_state)


def exchange(pieces, axis):
    return lax.all_to_all(pieces, axis, 0, 0, tiled=True)


def local(
    hidden,
    norm_gain,
    gate_weight,
    inner_weight,
    write_weight,
    read_weight,
    step_weight,
    conv_inner,
    conv_write,
    conv_read,
    step_bias,
    decay_log,
    skip_gain,
    group_gain,
    out_weight,
    state_inner,
    state_write,
    state_read,
    recurrent,
):
    write_weight, read_weight = jnp.swapaxes(write_weight, 1, 2), jnp.swapaxes(read_weight, 1, 2)
    state_inner, state_write, state_read = (
        jnp.swapaxes(s, 1, 2) for s in (state_inner, state_write, state_read)
    )
    recurrent = recurrent.reshape(2, 8, 128, 128)
    weights = (gate_weight, inner_weight, write_weight, read_weight, step_weight)

    first = pl.pallas_call(
        begin,
        name="begin",
        out_shape=jax.ShapeDtypeStruct((8, 128), F32),
        out_specs=pl.BlockSpec(memory_space=pltpu.VMEM),
        cost_estimate=pl.CostEstimate(flops=20000000000, bytes_accessed=0, transcendentals=0),
        compiler_params=pltpu.CompilerParams(vmem_limit_bytes=1024 * 1024),
    )()
    small = (conv_inner, conv_write, conv_read, step_bias, decay_log, skip_gain, group_gain)
    out, own, *small = call(
        lambda t, first, hidden, gain, gate, inner, write, read, step, *small: (
            *first_project(t, hidden, gain, gate, inner, write, read, step),
            *small,
        ),
        "first_project",
        (((64, 384), BF), ((8, 128), F32)) + tuple((a.shape, a.dtype) for a in small),
        first,
        hidden,
        norm_gain,
        *weights,
        *small,
        placed=True,
    )
    conv_inner, conv_write, conv_read, step_bias, decay_log, skip_gain, group_gain = small
    got = exchange(out.reshape(8, 8, 384), DP)
    message, parts, raw0 = call(
        first_states,
        "first_states",
        (((64, 8, 128), BF), ((32, 128), F32), ((8, 384), BF)),
        got,
        conv_inner,
        conv_write,
        conv_read,
        state_inner,
        state_write,
        state_read,
        step_bias,
        decay_log,
        write_weight,
        read_weight,
    )
    early = exchange(message, TP)
    message, turned, updated = scan_call(
        lambda got, parts, state, skip: first_scan(got, parts, state, skip),
        "first_scan",
        (((8, 8, 128), BF), ((40, 256), F32)),
        (early, parts, skip_gain),
        recurrent,
        None,
    )
    got = exchange(message, DP)
    (out,) = call(
        first_finish, "first_finish", (((64, 16, 128), BF),), got, group_gain, out_weight, write_weight, read_weight
    )
    middle = exchange(out, TP)
    (out,) = call(first_combine, "first_combine", (((64, 8, 128), BF),), middle, own, write_weight, read_weight)
    got = exchange(out, TP)
    out, own = call(
        second_project,
        "second_project",
        (((64, 640), BF), ((32, 128), F32)),
        got,
        norm_gain,
        *weights,
        early,
        middle,
        placed=True,
    )
    got = exchange(out.reshape(8, 8, 640), DP)
    message, raw1, second, updated = scan_call(
        second_scan,
        "second_scan",
        (((8, 8, 128), BF), ((8, 640), BF)),
        (got, turned, conv_inner, state_inner, step_bias, decay_log, skip_gain),
        recurrent,
        updated,
    )
    got = exchange(message, DP)
    (out,) = call(second_finish, "second_finish", (((8, 40, 128), BF),), got, group_gain, out_weight)
    got = exchange(out, Y)
    (out,) = call(second_scale, "second_scale", (((8, 32, 128), BF),), got)
    got = exchange(out, Z)
    (out,) = call(second_combine, "second_combine", (((8, 32, 128), BF),), got, own)
    got = exchange(out, Y)
    result, next_inner, next_write, next_read, updated = last_call(
        (((64, 512), BF), ((2, 3, 8, 128), BF), ((2, 3, 8, 32), BF), ((2, 3, 8, 32), BF)),
        (got, raw0, raw1, state_inner, state_write, state_read),
        second,
        updated,
    )
    return (
        result,
        jnp.swapaxes(next_inner, 1, 2),
        jnp.swapaxes(next_write, 1, 2),
        jnp.swapaxes(next_read, 1, 2),
        updated.reshape(2, 8, 2, 64, 128),
    )


def solution(mesh):
    finer = Mesh(mesh.devices.reshape(8, 8, 4, 2), ("tp_0", "tp_1", "dp_0", "dp_1"))
    placed = (
        P(None, DP),
        P(None, DP),
        P(None, DP, TP),
        P(None, DP, TP),
        P(None, DP, TP),
        P(None, DP, TP),
        P(None, DP, None),
        P(None, None, TP),
        P(None, None, TP),
        P(None, None, TP),
        P(None, TP),
        P(None, TP),
        P(None, TP),
        P(None, TP),
        P(None, TP, DP),
        P(None, DP, None, TP),
        P(None, DP, None, TP),
        P(None, DP, None, TP),
        P(None, DP, TP, None, None),
    )
    return jax.shard_map(
        local,
        mesh=finer,
        in_specs=placed,
        out_specs=(
            P(None, DP),
            P(None, DP, None, TP),
            P(None, DP, None, TP),
            P(None, DP, None, TP),
            P(None, DP, TP, None, None),
        ),
        check_vma=False,
    )
```

```python
import jax
import jax.numpy as jnp
from jax import lax
from jax.experimental import pallas as pl
from jax.experimental.pallas import tpu as pltpu
from jax.sharding import Mesh
from jax.sharding import PartitionSpec as P

D = 4096
DP = ("dp_0", "dp_1")
TP = ("tp_0", "tp_1")
Y = "tp_1"
Z = "tp_0"
EPS = 1e-06
BF = jnp.bfloat16
F32 = jnp.float32


def iota(shape, dim):
    return lax.broadcasted_iota(jnp.int32, shape, dim)


def dot(a, b):
    return lax.dot_general(a, b, (((1,), (0,)), ((), ())), preferred_element_type=F32)


def dot_rows(a, b):
    return lax.dot_general(a, b, (((1,), (1,)), ((), ())), preferred_element_type=F32)


def silu(a):
    return a * (1.0 / (1.0 + jnp.exp(-a)))


def rounded(a):
    return a.astype(BF).astype(F32)


def one_hot(test):
    return test.astype(F32).astype(BF)


def channel(k, group):
    return k // 2 * 32 + k % 2 * 16 + group


def to_groups(entry, blocks, pick):
    row, col = iota((512, 64), 0), iota((512, 64), 1)
    here = col == channel(entry(row % 8), row // 32)
    total = jnp.zeros((512, 128), F32)
    for b, block in enumerate(blocks):
        total = total + dot(one_hot(here & (pick(row % 8) == b)), block)
    return total


def quarters(weights):
    return [weights[:, 128 * q : 128 * q + 128] for q in range(4)]


def from_groups(*got):
    row, col = iota((512, 512), 0), iota((512, 512), 1)
    side = jnp.concatenate([g.reshape(512, 128) for g in got], axis=1)
    return dot(one_hot(col == row % 64 * 8 + row // 64), side).astype(BF)


def side_by_side(rows, first):
    return jnp.concatenate([rows[64 * j : 64 * j + 64] for j in range(first, first + 4)], axis=1)


def project(t, wide, gain, gate_w, inner_w, write_w, read_w, step_w, extra):
    scaled = (wide * gain).astype(BF)
    squares = jnp.sum(wide * wide, axis=1, keepdims=True)
    high = rounded(squares)
    vectors = dot_rows(scaled, jnp.concatenate([write_w, read_w], axis=0))
    step = dot(scaled, step_w).astype(BF)
    row, col = iota((128, 128), 0), iota((128, 128), 1)
    mine = ((col - 64 == row - 2 * t) & (col >= 64) & (col < 66)).astype(F32).astype(BF)
    lane = iota((64, 128), 1)
    third = jnp.concatenate([vectors, jnp.zeros((64, 64), F32)], axis=1) + dot(step, mine)
    third = jnp.where(lane == 66, high, jnp.where(lane == 67, squares - high, third))
    parts = [dot(scaled, gate_w), dot(scaled, inner_w), third]
    if extra is not None:
        parts.append(dot_rows(scaled, extra))
    return jnp.concatenate(parts, axis=1).astype(BF)


def first_project(t, hidden, gain, gate_w, inner_w, write_w, read_w, step_w):
    out = project(
        t, hidden.astype(F32), gain[0:1], gate_w[0], inner_w[0], write_w[0], read_w[0], step_w[0], None
    )
    pick = (iota((8, 512), 1) == iota((8, 512), 0) + 8 * t).astype(F32).astype(BF)
    own = jnp.concatenate([dot_rows(pick, hidden), jnp.zeros((8, 64), F32)], axis=1)
    return out, own


def turned_back(got):
    return jnp.transpose(got.reshape(512, 128).astype(F32))[:64]


def second_project(t, got, gain, gate_w, inner_w, write_w, read_w, step_w, early):
    wide = turned_back(got)
    both = from_groups(early[:, :8], early[:, 8:], got)
    early, middle, late = both[:, :128], both[:, 128:256], both[:, 256:]
    blocks = [late[64 * i : 64 * i + 64] for i in range(8)]
    low = iota((64, 128), 1) < 64
    pairs = []
    for q in range(4):
        even, odd = blocks[2 * q].astype(F32), blocks[2 * q + 1].astype(F32)
        even = jnp.concatenate([even[:, 64:], even[:, :64]], axis=1)
        pairs.append(jnp.where(low, even, odd).astype(BF))
    later = jnp.concatenate(
        [
            side_by_side(early, 0),
            side_by_side(early, 4),
            side_by_side(middle, 0),
            jnp.concatenate(pairs, axis=1),
        ],
        axis=0,
    )
    out = project(t, wide, gain[1:2], gate_w[1], inner_w[1], write_w[1], read_w[1], step_w[1], later)
    row, col = iota((32, 512), 0), iota((32, 512), 1)
    first = t % 8 * 32
    rows = got.reshape(512, 128)
    own = [dot(one_hot(col == row + first + half), rows)[:, :64] for half in (0, 256)]
    return out, jnp.concatenate(own, axis=1)


def arrive(got):
    total = got[0].astype(F32)
    for k in range(1, 8):
        total = total + got[k].astype(F32)
    squares = total[:, 322:323] + total[:, 323:324]
    return (total * lax.rsqrt(squares / D + EPS)).astype(BF)


def convolve(rows, fresh, taps):
    total = fresh.astype(F32) * taps[3:4].astype(F32)
    for k in range(3):
        total = total + rows[k].astype(F32) * taps[k : k + 1].astype(F32)
    return silu(total)


def by_head(pair):
    return jnp.where(iota((8, 128), 1) < 64, pair[:, 0:1], pair[:, 1:2])


def local_parts(raw, number, conv_inner, state_inner, bias, decay):
    inner = convolve(state_inner[number], raw[:, 128:256], conv_inner[number])
    shifted = raw[:, 320:322].astype(F32) + bias[number : number + 1]
    step = jnp.maximum(shifted, 0.0) + jnp.log1p(jnp.exp(-jnp.abs(shifted)))
    retain = jnp.exp(-step * jnp.exp(decay[number : number + 1]))
    gate = silu(raw[:, :128].astype(F32))
    return inner, by_head(step), by_head(retain), gate


def next_rows(state, fresh):
    return jnp.concatenate([state[1:], fresh[None]], axis=0)


def first_states(got, conv_inner, conv_write, conv_read, state_inner, state_write, state_read, bias, decay, write_w, read_w):
    raw = arrive(got)
    inner, step, retain, gate = local_parts(raw, 0, conv_inner, state_inner, bias, decay)
    vec_state = jnp.concatenate([state_write, state_read], axis=3).astype(F32)
    vec_taps = jnp.concatenate([conv_write, conv_read], axis=2).astype(F32)
    acts = convolve(vec_state[0], raw[:, 256:320], vec_taps[0])
    extras = jnp.concatenate(
        [
            acts,
            vec_taps[1],
            jnp.zeros((4, 64), F32),
            vec_state[1].reshape(24, 64),
            jnp.zeros((88, 64), F32),
        ],
        axis=0,
    ).astype(BF)
    row, col = iota((512, 64), 0), iota((512, 64), 1)
    spread = one_hot((row % 8 >= 4) & (col == channel(row % 8 - 4, row // 32)))
    weights = jnp.concatenate([write_w[1], read_w[1]], axis=0)
    blocks = quarters(weights)
    early = to_groups(lambda j: j // 4, blocks, lambda j: j % 4)
    late = to_groups(lambda j: 0 * j + 2, blocks, lambda j: j) + dot_rows(spread, extras)
    message = [m.astype(BF).reshape(64, 8, 128) for m in (early, late)]
    message = jnp.concatenate(message, axis=1)
    return message, jnp.concatenate([inner, step, retain, gate], axis=0), raw


def sort_vectors(acts):
    row, col = iota((256, 256), 0), iota((256, 256), 1)
    order = one_hot(row == col // 128 * 128 + col % 2 * 64 + col % 128 // 2)
    both = dot(acts.astype(BF), order)
    return both[:, :128], both[:, 128:]


def scan_step(recurrent, inner, step, retain, gate, write_vec, read_vec, skip):
    turned = jnp.transpose(jnp.concatenate([step * inner, retain, jnp.zeros((112, 128), F32)], axis=0))
    lane = iota((128, 128), 1)
    updated, reads = [], jnp.zeros((128, 128), F32)
    for b in range(8):
        new = turned[:, 8 + b : 9 + b] * recurrent[b] + turned[:, b : b + 1] * write_vec[b : b + 1]
        updated.append(new)
        reads = jnp.where(lane == b, jnp.sum(new * read_vec[b : b + 1], axis=1, keepdims=True), reads)
    readout = jnp.transpose(reads)[:8] + by_head(jnp.broadcast_to(skip, (8, 2))) * inner
    gated = (readout * gate).astype(BF)
    return updated, jnp.broadcast_to(gated[None], (8, 8, 128))


def first_scan(got, parts, recurrent, skip):
    row, col = iota((256, 512), 0), iota((256, 512), 1)
    extras = dot(one_hot(col == row % 64 * 8 + 4 + row // 64), got[:, 8:].reshape(512, 128))
    turned = jnp.transpose(extras)[:40]
    write_vec, read_vec = sort_vectors(turned[:8])
    updated, message = scan_step(
        recurrent[0], parts[:8], parts[8:16], parts[16:24], parts[24:], write_vec, read_vec, skip[0:1]
    )
    return message, turned, updated


def second_scan(got, turned, conv_inner, state_inner, bias, decay, recurrent, skip):
    raw = arrive(got)
    inner, step, retain, gate = local_parts(raw, 1, conv_inner, state_inner, bias, decay)
    rows = turned[16:40].reshape(3, 8, 256)
    acts = convolve(rows, raw[:, 384:], turned[8:12])
    write_vec, read_vec = sort_vectors(acts)
    updated, message = scan_step(recurrent[1], inner, step, retain, gate, write_vec, read_vec, skip[1:2])
    return message, raw, updated


def partial(number, got, gain, out_w):
    wide = got.reshape(64, 128).astype(F32)
    squares = jnp.sum(wide * wide, axis=1, keepdims=True)
    part = dot((wide * gain[number : number + 1]).astype(BF), out_w[number])
    return jnp.transpose(jnp.concatenate([part, jnp.broadcast_to(squares, (64, 512))], axis=0))


def first_finish(got, gain, out_w):
    turned = partial(0, got, gain, out_w)
    high = rounded(turned)
    lane, row = iota((512, 128), 1), iota((512, 128), 0)
    out = jnp.where((lane < 64) | (row % 8 < 4), turned, turned - high).astype(BF)
    return (out.reshape(64, 8, 128),)


def first_combine(got, own, write_w, read_w):
    some = got.astype(F32).reshape(16, 4, 8, 128)
    some = some[:, 0] + some[:, 1] + some[:, 2] + some[:, 3]
    both = some + jnp.concatenate([some[:, 4:], some[:, :4]], axis=1)
    factor = lax.rsqrt(both / 512 + EPS)
    factor = jnp.concatenate([factor[:, :, 64:], factor[:, :, :64]], axis=2)
    new = own + jnp.sum(some * factor, axis=0)
    weights = jnp.concatenate([write_w[1], read_w[1]], axis=0)
    rolled = jnp.concatenate([weights[:, 64:], weights[:, :64]], axis=1)
    odd, even = quarters(weights), quarters(rolled)
    blocks = [odd[i // 2] if i % 2 else even[(i // 2 + 3) % 4] for i in range(8)]
    beside = to_groups(lambda j: 0 * j + 3, blocks, lambda j: j).reshape(64, 8, 128)
    low = iota((64, 8, 128), 2) < 64
    return (jnp.where(low, jnp.broadcast_to(new[None], (64, 8, 128)), beside).astype(BF),)


def second_finish(got, gain, out_w):
    turned = partial(1, got, gain, out_w)
    out = jnp.concatenate([turned[:256, :64], turned[256:, :64]], axis=1)
    squares = jnp.concatenate([turned[:8, 64:], turned[:8, 64:]], axis=1)
    high = rounded(squares)
    squares = jnp.where(iota((8, 128), 0) < 4, high, squares - high)
    squares = jnp.broadcast_to(squares[None], (8, 8, 128))
    return (jnp.concatenate([out.reshape(8, 32, 128), squares], axis=1).astype(BF),)


def second_scale(got):
    total = jnp.zeros((32, 128), F32)
    for half in (0, 4):
        some = got[half].astype(F32)
        for k in range(1, 4):
            some = some + got[half + k].astype(F32)
        squares = some[32:33] + some[36:37]
        total = total + some[:32] * lax.rsqrt(squares / 512 + EPS)
    return (jnp.broadcast_to(total.astype(BF)[None], (8, 32, 128)),)


def second_combine(got, own):
    for k in range(8):
        own = own + got[k].astype(F32)
    return (jnp.broadcast_to(own.astype(BF)[None], (8, 32, 128)),)


def last(got, raw0, raw1, state_inner, state_write, state_read):
    turned = jnp.transpose(got.reshape(256, 128).astype(F32))
    outs = [jnp.concatenate([turned[:64], turned[64:]], axis=1).astype(BF)]
    for state, low, high in ((state_inner, 128, 256), (state_write, 256, 288), (state_read, 288, 320)):
        rows = [next_rows(state[0], raw0[:, low:high])[None], next_rows(state[1], raw1[:, low:high])[None]]
        outs.append(jnp.concatenate(rows, axis=0))
    return tuple(outs)


def call(fn, name, outs, *args, placed=False):
    n_in = len(args)

    def kernel(*refs):
        values = [r[...] for r in refs[:n_in]]
        dest = refs[n_in:]
        if placed:
            values = [lax.axis_index(Z) * 8 + lax.axis_index(Y)] + values
        for ref, value in zip(dest, fn(*values)):
            ref[...] = value

    whole = pl.BlockSpec(memory_space=pltpu.VMEM)
    specs = [whole] * n_in
    return pl.pallas_call(
        kernel,
        name=name,
        out_shape=tuple(jax.ShapeDtypeStruct(s, d) for s, d in outs),
        in_specs=specs,
        out_specs=tuple(whole for _ in outs),
        compiler_params=pltpu.CompilerParams(vmem_limit_bytes=16 * 1024 * 1024),
    )(*args)


def begin(out_ref):
    out_ref[...] = jnp.zeros((8, 128), F32)


def start_copies(source, dest, sems):
    copies = [pltpu.make_async_copy(source.at[b], dest.at[b], sems.at[b]) for b in range(8)]
    for copy in copies:
        copy.start()
    return copies


def scan_call(fn, name, outs, args, recurrent, earlier):
    n_in = len(args)

    def kernel(*refs):
        values = [r[...] for r in refs[:n_in]]
        state = refs[n_in]
        if earlier is None:
            dest = refs[n_in + 1 :]
        else:
            dest, whole_ref, sem = refs[n_in + 2 : -2], refs[-2], refs[-1]
            copies = start_copies(refs[n_in + 1], whole_ref.at[0], sem)
        results = fn(*values[:-1], state, values[-1])
        for ref, value in zip(dest[:-1], results[:-1]):
            ref[...] = value
        for b in range(8):
            dest[-1][b] = results[-1][b]
        if earlier is not None:
            for copy in copies:
                copy.wait()

    whole = pl.BlockSpec(memory_space=pltpu.VMEM)
    specs = [whole] * (n_in + 1 + (earlier is not None))
    operands = (*args, recurrent) + (() if earlier is None else (earlier,))
    outs = (*outs, ((8, 128, 128), F32))
    out_specs = [whole] * len(outs)
    if earlier is not None:
        outs = (*outs, ((2, 8, 128, 128), F32))
        out_specs.append(pl.BlockSpec(memory_space=pl.ANY))
    return pl.pallas_call(
        kernel,
        name=name,
        out_shape=tuple(jax.ShapeDtypeStruct(s, d) for s, d in outs),
        in_specs=specs,
        out_specs=tuple(out_specs),
        scratch_shapes=[] if earlier is None else [pltpu.SemaphoreType.DMA((8,))],
        compiler_params=pltpu.CompilerParams(vmem_limit_bytes=16 * 1024 * 1024),
    )(*operands)


def last_call(outs, args, state, whole_state):
    n_in = len(args)

    def kernel(*refs):
        state_ref, dest, whole_ref, sem = refs[n_in], refs[n_in + 2 : -2], refs[-2], refs[-1]
        copies = start_copies(state_ref, whole_ref.at[1], sem)
        for ref, value in zip(dest, last(*[r[...] for r in refs[:n_in]])):
            ref[...] = value
        for copy in copies:
            copy.wait()

    whole, anywhere = pl.BlockSpec(memory_space=pltpu.VMEM), pl.BlockSpec(memory_space=pl.ANY)
    return pl.pallas_call(
        kernel,
        name="last",
        out_shape=tuple(jax.ShapeDtypeStruct(s, d) for s, d in outs)
        + (jax.ShapeDtypeStruct(whole_state.shape, F32),),
        in_specs=[whole] * (n_in + 1) + [anywhere],
        out_specs=tuple(whole for _ in outs) + (anywhere,),
        input_output_aliases={n_in + 1: len(outs)},
        scratch_shapes=[pltpu.SemaphoreType.DMA((8,))],
        compiler_params=pltpu.CompilerParams(vmem_limit_bytes=16 * 1024 * 1024),
    )(*args, state, whole_state)


def exchange(pieces, axis):
    return lax.all_to_all(pieces, axis, 0, 0, tiled=True)


def local(
    hidden,
    norm_gain,
    gate_weight,
    inner_weight,
    write_weight,
    read_weight,
    step_weight,
    conv_inner,
    conv_write,
    conv_read,
    step_bias,
    decay_log,
    skip_gain,
    group_gain,
    out_weight,
    state_inner,
    state_write,
    state_read,
    recurrent,
):
    write_weight, read_weight = jnp.swapaxes(write_weight, 1, 2), jnp.swapaxes(read_weight, 1, 2)
    state_inner, state_write, state_read = (
        jnp.swapaxes(s, 1, 2) for s in (state_inner, state_write, state_read)
    )
    recurrent = recurrent.reshape(2, 8, 128, 128)
    weights = (gate_weight, inner_weight, write_weight, read_weight, step_weight)

    first = pl.pallas_call(
        begin,
        name="begin",
        out_shape=jax.ShapeDtypeStruct((8, 128), F32),
        out_specs=pl.BlockSpec(memory_space=pltpu.VMEM),
        cost_estimate=pl.CostEstimate(flops=20000000000, bytes_accessed=0, transcendentals=0),
        compiler_params=pltpu.CompilerParams(vmem_limit_bytes=1024 * 1024),
    )()
    small = (conv_inner, conv_write, conv_read, step_bias, decay_log, skip_gain, group_gain)
    small = (*small, state_inner, state_write, state_read)
    out, own, *small = call(
        lambda t, first, hidden, gain, gate, inner, write, read, step, *small: (
            *first_project(t, hidden, gain, gate, inner, write, read, step),
            *small,
        ),
        "first_project",
        (((64, 384), BF), ((8, 128), F32)) + tuple((a.shape, a.dtype) for a in small),
        first,
        hidden,
        norm_gain,
        *weights,
        *small,
        placed=True,
    )
    conv_inner, conv_write, conv_read, step_bias, decay_log, skip_gain, group_gain = small[:7]
    state_inner, state_write, state_read = small[7:]
    got = exchange(out.reshape(8, 8, 384), DP)
    message, parts, raw0 = call(
        first_states,
        "first_states",
        (((64, 16, 128), BF), ((32, 128), F32), ((8, 384), BF)),
        got,
        conv_inner,
        conv_write,
        conv_read,
        state_inner,
        state_write,
        state_read,
        step_bias,
        decay_log,
        write_weight,
        read_weight,
    )
    early = exchange(message, TP)
    message, turned, updated = scan_call(
        lambda got, parts, state, skip: first_scan(got, parts, state, skip),
        "first_scan",
        (((8, 8, 128), BF), ((40, 256), F32)),
        (early, parts, skip_gain),
        recurrent,
        None,
    )
    got = exchange(message, DP)
    (out,) = call(first_finish, "first_finish", (((64, 8, 128), BF),), got, group_gain, out_weight)
    got = exchange(out, TP)
    (out,) = call(first_combine, "first_combine", (((64, 8, 128), BF),), got, own, write_weight, read_weight)
    got = exchange(out, TP)
    out, own = call(
        second_project,
        "second_project",
        (((64, 640), BF), ((32, 128), F32)),
        got,
        norm_gain,
        *weights,
        early,
        placed=True,
    )
    got = exchange(out.reshape(8, 8, 640), DP)
    message, raw1, second, updated = scan_call(
        second_scan,
        "second_scan",
        (((8, 8, 128), BF), ((8, 640), BF)),
        (got, turned, conv_inner, state_inner, step_bias, decay_log, skip_gain),
        recurrent,
        updated,
    )
    got = exchange(message, DP)
    (out,) = call(second_finish, "second_finish", (((8, 40, 128), BF),), got, group_gain, out_weight)
    got = exchange(out, Y)
    (out,) = call(second_scale, "second_scale", (((8, 32, 128), BF),), got)
    got = exchange(out, Z)
    (out,) = call(second_combine, "second_combine", (((8, 32, 128), BF),), got, own)
    got = exchange(out, Y)
    result, next_inner, next_write, next_read, updated = last_call(
        (((64, 512), BF), ((2, 3, 8, 128), BF), ((2, 3, 8, 32), BF), ((2, 3, 8, 32), BF)),
        (got, raw0, raw1, state_inner, state_write, state_read),
        second,
        updated,
    )
    return (
        result,
        jnp.swapaxes(next_inner, 1, 2),
        jnp.swapaxes(next_write, 1, 2),
        jnp.swapaxes(next_read, 1, 2),
        updated.reshape(2, 8, 2, 64, 128),
    )


def solution(mesh):
    finer = Mesh(mesh.devices.reshape(8, 8, 4, 2), ("tp_0", "tp_1", "dp_0", "dp_1"))
    placed = (
        P(None, DP),
        P(None, DP),
        P(None, DP, TP),
        P(None, DP, TP),
        P(None, DP, TP),
        P(None, DP, TP),
        P(None, DP, None),
        P(None, None, TP),
        P(None, None, TP),
        P(None, None, TP),
        P(None, TP),
        P(None, TP),
        P(None, TP),
        P(None, TP),
        P(None, TP, DP),
        P(None, DP, None, TP),
        P(None, DP, None, TP),
        P(None, DP, None, TP),
        P(None, DP, TP, None, None),
    )
    return jax.shard_map(
        local,
        mesh=finer,
        in_specs=placed,
        out_specs=(
            P(None, DP),
            P(None, DP, None, TP),
            P(None, DP, None, TP),
            P(None, DP, None, TP),
            P(None, DP, TP, None, None),
        ),
        check_vma=False,
    )
```

```python
import jax
import jax.numpy as jnp
from jax import lax
from jax.experimental import pallas as pl
from jax.experimental.pallas import tpu as pltpu
from jax.sharding import Mesh
from jax.sharding import PartitionSpec as P

D = 4096
DP = ("dp_0", "dp_1")
TP = ("tp_0", "tp_1")
Y = "tp_1"
Z = "tp_0"
EPS = 1e-06
BF = jnp.bfloat16
F32 = jnp.float32


def iota(shape, dim):
    return lax.broadcasted_iota(jnp.int32, shape, dim)


def dot(a, b):
    return lax.dot_general(a, b, (((1,), (0,)), ((), ())), preferred_element_type=F32)


def dot_rows(a, b):
    return lax.dot_general(a, b, (((1,), (1,)), ((), ())), preferred_element_type=F32)


def silu(a):
    return a * (1.0 / (1.0 + jnp.exp(-a)))


def rounded(a):
    return a.astype(BF).astype(F32)


def one_hot(test):
    return test.astype(F32).astype(BF)


def channel(k, group):
    return k // 2 * 32 + k % 2 * 16 + group


def to_groups(entry, blocks, pick):
    row, col = iota((512, 64), 0), iota((512, 64), 1)
    here = col == channel(entry(row % 8), row // 32)
    total = jnp.zeros((512, 128), F32)
    for b, block in enumerate(blocks):
        total = total + dot(one_hot(here & (pick(row % 8) == b)), block)
    return total


def quarters(weights):
    return [weights[:, 128 * q : 128 * q + 128] for q in range(4)]


def from_groups(*got):
    row, col = iota((512, 512), 0), iota((512, 512), 1)
    side = jnp.concatenate([g.reshape(512, 128) for g in got], axis=1)
    return dot(one_hot(col == row % 64 * 8 + row // 64), side).astype(BF)


def side_by_side(rows, first):
    return jnp.concatenate([rows[64 * j : 64 * j + 64] for j in range(first, first + 4)], axis=1)


def spread(first, write_w, read_w):
    weights = jnp.concatenate([write_w[1], read_w[1]], axis=0)
    rolled = jnp.concatenate([weights[:, 64:], weights[:, :64]], axis=1)
    odd, even = quarters(weights), quarters(rolled)
    halves = [odd[i // 2] if i % 2 else even[(i // 2 + 3) % 4] for i in range(8)]
    early = to_groups(lambda j: j // 4, odd, lambda j: j % 4)
    late = to_groups(lambda j: 0 * j + 2, odd, lambda j: j)
    message = jnp.concatenate([m.astype(BF).reshape(64, 8, 128) for m in (early, late)], axis=1)
    beside = to_groups(lambda j: 0 * j + 3, halves, lambda j: j)
    return message, beside.astype(BF).reshape(64, 8, 128)


def project(t, wide, gain, gate_w, inner_w, write_w, read_w, step_w, extra):
    scaled = (wide * gain).astype(BF)
    squares = jnp.sum(wide * wide, axis=1, keepdims=True)
    high = rounded(squares)
    vectors = dot_rows(scaled, jnp.concatenate([write_w, read_w], axis=0))
    step = dot(scaled, step_w).astype(BF)
    row, col = iota((128, 128), 0), iota((128, 128), 1)
    mine = ((col - 64 == row - 2 * t) & (col >= 64) & (col < 66)).astype(F32).astype(BF)
    lane = iota((64, 128), 1)
    third = jnp.concatenate([vectors, jnp.zeros((64, 64), F32)], axis=1) + dot(step, mine)
    third = jnp.where(lane == 66, high, jnp.where(lane == 67, squares - high, third))
    parts = [dot(scaled, gate_w), dot(scaled, inner_w), third]
    if extra is not None:
        parts.append(dot_rows(scaled, extra))
    return jnp.concatenate(parts, axis=1).astype(BF)


def first_project(t, hidden, gain, gate_w, inner_w, write_w, read_w, step_w):
    out = project(
        t, hidden.astype(F32), gain[0:1], gate_w[0], inner_w[0], write_w[0], read_w[0], step_w[0], None
    )
    pick = (iota((8, 512), 1) == iota((8, 512), 0) + 8 * t).astype(F32).astype(BF)
    own = jnp.concatenate([dot_rows(pick, hidden), jnp.zeros((8, 64), F32)], axis=1)
    return out, own


def turned_back(got):
    return jnp.transpose(got.reshape(512, 128).astype(F32))[:64]


def second_project(t, got, gain, gate_w, inner_w, write_w, read_w, step_w, early):
    wide = turned_back(got)
    both = from_groups(early[:, :8], early[:, 8:], got)
    early, middle, late = both[:, :128], both[:, 128:256], both[:, 256:]
    blocks = [late[64 * i : 64 * i + 64] for i in range(8)]
    low = iota((64, 128), 1) < 64
    pairs = []
    for q in range(4):
        even, odd = blocks[2 * q].astype(F32), blocks[2 * q + 1].astype(F32)
        even = jnp.concatenate([even[:, 64:], even[:, :64]], axis=1)
        pairs.append(jnp.where(low, even, odd).astype(BF))
    later = jnp.concatenate(
        [
            side_by_side(early, 0),
            side_by_side(early, 4),
            side_by_side(middle, 0),
            jnp.concatenate(pairs, axis=1),
        ],
        axis=0,
    )
    out = project(t, wide, gain[1:2], gate_w[1], inner_w[1], write_w[1], read_w[1], step_w[1], later)
    row, col = iota((32, 512), 0), iota((32, 512), 1)
    first = t % 8 * 32
    rows = got.reshape(512, 128)
    own = [dot(one_hot(col == row + first + half), rows)[:, :64] for half in (0, 256)]
    return out, jnp.concatenate(own, axis=1)


def arrive(got):
    total = got[0].astype(F32)
    for k in range(1, 8):
        total = total + got[k].astype(F32)
    squares = total[:, 322:323] + total[:, 323:324]
    return (total * lax.rsqrt(squares / D + EPS)).astype(BF)


def convolve(rows, fresh, taps):
    total = fresh.astype(F32) * taps[3:4].astype(F32)
    for k in range(3):
        total = total + rows[k].astype(F32) * taps[k : k + 1].astype(F32)
    return silu(total)


def by_head(pair):
    return jnp.where(iota((8, 128), 1) < 64, pair[:, 0:1], pair[:, 1:2])


def local_parts(raw, number, conv_inner, state_inner, bias, decay):
    inner = convolve(state_inner[number], raw[:, 128:256], conv_inner[number])
    shifted = raw[:, 320:322].astype(F32) + bias[number : number + 1]
    step = jnp.maximum(shifted, 0.0) + jnp.log1p(jnp.exp(-jnp.abs(shifted)))
    retain = jnp.exp(-step * jnp.exp(decay[number : number + 1]))
    gate = silu(raw[:, :128].astype(F32))
    return inner, by_head(step), by_head(retain), gate


def next_rows(state, fresh):
    return jnp.concatenate([state[1:], fresh[None]], axis=0)


def first_states(got, conv_inner, conv_write, conv_read, state_inner, state_write, state_read, bias, decay, early):
    raw = arrive(got)
    inner, step, retain, gate = local_parts(raw, 0, conv_inner, state_inner, bias, decay)
    vec_state = jnp.concatenate([state_write, state_read], axis=3).astype(F32)
    vec_taps = jnp.concatenate([conv_write, conv_read], axis=2).astype(F32)
    acts = convolve(vec_state[0], raw[:, 256:320], vec_taps[0])
    extras = jnp.concatenate(
        [
            acts,
            vec_taps[1],
            jnp.zeros((4, 64), F32),
            vec_state[1].reshape(24, 64),
            jnp.zeros((88, 64), F32),
        ],
        axis=0,
    ).astype(BF)
    row, col = iota((512, 64), 0), iota((512, 64), 1)
    here = one_hot((row % 8 >= 4) & (col == channel(row % 8 - 4, row // 32)))
    late = dot_rows(here, extras).reshape(64, 8, 128) + early[:, 8:].astype(F32)
    message = jnp.concatenate([early[:, :8], late.astype(BF)], axis=1)
    return message, jnp.concatenate([inner, step, retain, gate], axis=0), raw


def sort_vectors(acts):
    row, col = iota((256, 256), 0), iota((256, 256), 1)
    order = one_hot(row == col // 128 * 128 + col % 2 * 64 + col % 128 // 2)
    both = dot(acts.astype(BF), order)
    return both[:, :128], both[:, 128:]


def scan_step(recurrent, inner, step, retain, gate, write_vec, read_vec, skip):
    turned = jnp.transpose(jnp.concatenate([step * inner, jnp.zeros((120, 128), F32)], axis=0))
    lane = iota((128, 128), 1)
    updated, reads = [], jnp.zeros((128, 128), F32)
    for b in range(8):
        kept = [jnp.broadcast_to(retain[b : b + 1, c : c + 1], (64, 128)) for c in (0, 64)]
        new = jnp.concatenate(kept, axis=0) * recurrent[b] + turned[:, b : b + 1] * write_vec[b : b + 1]
        updated.append(new)
        reads = jnp.where(lane == b, jnp.sum(new * read_vec[b : b + 1], axis=1, keepdims=True), reads)
    readout = jnp.transpose(reads)[:8] + by_head(jnp.broadcast_to(skip, (8, 2))) * inner
    gated = (readout * gate).astype(BF)
    return updated, jnp.broadcast_to(gated[None], (8, 8, 128))


def first_scan(got, parts, recurrent, skip):
    row, col = iota((256, 512), 0), iota((256, 512), 1)
    extras = dot(one_hot(col == row % 64 * 8 + 4 + row // 64), got[:, 8:].reshape(512, 128))
    turned = jnp.transpose(extras)[:40]
    write_vec, read_vec = sort_vectors(turned[:8])
    updated, message = scan_step(
        recurrent[0], parts[:8], parts[8:16], parts[16:24], parts[24:], write_vec, read_vec, skip[0:1]
    )
    return message, turned, updated


def second_scan(got, turned, conv_inner, state_inner, bias, decay, recurrent, skip):
    raw = arrive(got)
    inner, step, retain, gate = local_parts(raw, 1, conv_inner, state_inner, bias, decay)
    rows = turned[16:40].reshape(3, 8, 256)
    acts = convolve(rows, raw[:, 384:], turned[8:12])
    write_vec, read_vec = sort_vectors(acts)
    updated, message = scan_step(recurrent[1], inner, step, retain, gate, write_vec, read_vec, skip[1:2])
    return message, raw, updated


def partial(number, got, gain, out_w):
    wide = got.reshape(64, 128).astype(F32)
    squares = jnp.sum(wide * wide, axis=1, keepdims=True)
    part = dot((wide * gain[number : number + 1]).astype(BF), out_w[number])
    return jnp.transpose(jnp.concatenate([part, jnp.broadcast_to(squares, (64, 512))], axis=0))


def first_finish(got, gain, out_w):
    turned = partial(0, got, gain, out_w)
    high = rounded(turned)
    lane, row = iota((512, 128), 1), iota((512, 128), 0)
    out = jnp.where((lane < 64) | (row % 8 < 4), turned, turned - high).astype(BF)
    return (out.reshape(64, 8, 128),)


def first_combine(got, own, beside):
    some = got.astype(F32).reshape(16, 4, 8, 128)
    some = some[:, 0] + some[:, 1] + some[:, 2] + some[:, 3]
    both = some + jnp.concatenate([some[:, 4:], some[:, :4]], axis=1)
    factor = lax.rsqrt(both / 512 + EPS)
    factor = jnp.concatenate([factor[:, :, 64:], factor[:, :, :64]], axis=2)
    new = own + jnp.sum(some * factor, axis=0)
    low = iota((64, 8, 128), 2) < 64
    return (jnp.where(low, jnp.broadcast_to(new[None], (64, 8, 128)), beside.astype(F32)).astype(BF),)


def second_finish(got, gain, out_w):
    turned = partial(1, got, gain, out_w)
    out = jnp.concatenate([turned[:256, :64], turned[256:, :64]], axis=1)
    squares = jnp.concatenate([turned[:8, 64:], turned[:8, 64:]], axis=1)
    high = rounded(squares)
    squares = jnp.where(iota((8, 128), 0) < 4, high, squares - high)
    squares = jnp.broadcast_to(squares[None], (8, 8, 128))
    return (jnp.concatenate([out.reshape(8, 32, 128), squares], axis=1).astype(BF),)


def second_scale(got):
    total = jnp.zeros((32, 128), F32)
    for half in (0, 4):
        some = got[half].astype(F32)
        for k in range(1, 4):
            some = some + got[half + k].astype(F32)
        squares = some[32:33] + some[36:37]
        total = total + some[:32] * lax.rsqrt(squares / 512 + EPS)
    return (jnp.broadcast_to(total.astype(BF)[None], (8, 32, 128)),)


def second_combine(got, own):
    for k in range(8):
        own = own + got[k].astype(F32)
    return (jnp.broadcast_to(own.astype(BF)[None], (8, 32, 128)),)


def last(got, raw0, raw1, state_inner, state_write, state_read):
    turned = jnp.transpose(got.reshape(256, 128).astype(F32))
    outs = [jnp.concatenate([turned[:64], turned[64:]], axis=1).astype(BF)]
    for state, low, high in ((state_inner, 128, 256), (state_write, 256, 288), (state_read, 288, 320)):
        rows = [next_rows(state[0], raw0[:, low:high])[None], next_rows(state[1], raw1[:, low:high])[None]]
        outs.append(jnp.concatenate(rows, axis=0))
    return tuple(outs)


def call(fn, name, outs, *args, placed=False):
    n_in = len(args)

    def kernel(*refs):
        values = [r[...] for r in refs[:n_in]]
        dest = refs[n_in:]
        if placed:
            values = [lax.axis_index(Z) * 8 + lax.axis_index(Y)] + values
        for ref, value in zip(dest, fn(*values)):
            ref[...] = value

    whole = pl.BlockSpec(memory_space=pltpu.VMEM)
    specs = [whole] * n_in
    return pl.pallas_call(
        kernel,
        name=name,
        out_shape=tuple(jax.ShapeDtypeStruct(s, d) for s, d in outs),
        in_specs=specs,
        out_specs=tuple(whole for _ in outs),
        compiler_params=pltpu.CompilerParams(vmem_limit_bytes=16 * 1024 * 1024),
    )(*args)


def begin(out_ref):
    out_ref[...] = jnp.zeros((8, 128), F32)


def start_copies(source, dest, sems):
    copies = [pltpu.make_async_copy(source.at[b], dest.at[b], sems.at[b]) for b in range(8)]
    for copy in copies:
        copy.start()
    return copies


def scan_call(fn, name, outs, args, recurrent, earlier):
    n_in = len(args)

    def kernel(*refs):
        values = [r[...] for r in refs[:n_in]]
        state = refs[n_in]
        if earlier is None:
            dest = refs[n_in + 1 :]
        else:
            dest, whole_ref, sem = refs[n_in + 2 : -2], refs[-2], refs[-1]
            copies = start_copies(refs[n_in + 1], whole_ref.at[0], sem)
        results = fn(*values[:-1], state, values[-1])
        for ref, value in zip(dest[:-1], results[:-1]):
            ref[...] = value
        for b in range(8):
            dest[-1][b] = results[-1][b]
        if earlier is not None:
            for copy in copies:
                copy.wait()

    whole = pl.BlockSpec(memory_space=pltpu.VMEM)
    specs = [whole] * (n_in + 1 + (earlier is not None))
    operands = (*args, recurrent) + (() if earlier is None else (earlier,))
    outs = (*outs, ((8, 128, 128), F32))
    out_specs = [whole] * len(outs)
    if earlier is not None:
        outs = (*outs, ((2, 8, 128, 128), F32))
        out_specs.append(pl.BlockSpec(memory_space=pl.ANY))
    return pl.pallas_call(
        kernel,
        name=name,
        out_shape=tuple(jax.ShapeDtypeStruct(s, d) for s, d in outs),
        in_specs=specs,
        out_specs=tuple(out_specs),
        scratch_shapes=[] if earlier is None else [pltpu.SemaphoreType.DMA((8,))],
        compiler_params=pltpu.CompilerParams(vmem_limit_bytes=16 * 1024 * 1024),
    )(*operands)


def last_call(outs, args, state, whole_state):
    n_in = len(args)

    def kernel(*refs):
        state_ref, dest, whole_ref, sem = refs[n_in], refs[n_in + 2 : -2], refs[-2], refs[-1]
        copies = start_copies(state_ref, whole_ref.at[1], sem)
        for ref, value in zip(dest, last(*[r[...] for r in refs[:n_in]])):
            ref[...] = value
        for copy in copies:
            copy.wait()

    whole, anywhere = pl.BlockSpec(memory_space=pltpu.VMEM), pl.BlockSpec(memory_space=pl.ANY)
    return pl.pallas_call(
        kernel,
        name="last",
        out_shape=tuple(jax.ShapeDtypeStruct(s, d) for s, d in outs)
        + (jax.ShapeDtypeStruct(whole_state.shape, F32),),
        in_specs=[whole] * (n_in + 1) + [anywhere],
        out_specs=tuple(whole for _ in outs) + (anywhere,),
        input_output_aliases={n_in + 1: len(outs)},
        scratch_shapes=[pltpu.SemaphoreType.DMA((8,))],
        compiler_params=pltpu.CompilerParams(vmem_limit_bytes=16 * 1024 * 1024),
    )(*args, state, whole_state)


def exchange(pieces, axis):
    return lax.all_to_all(pieces, axis, 0, 0, tiled=True)


def local(
    hidden,
    norm_gain,
    gate_weight,
    inner_weight,
    write_weight,
    read_weight,
    step_weight,
    conv_inner,
    conv_write,
    conv_read,
    step_bias,
    decay_log,
    skip_gain,
    group_gain,
    out_weight,
    state_inner,
    state_write,
    state_read,
    recurrent,
):
    write_weight, read_weight = jnp.swapaxes(write_weight, 1, 2), jnp.swapaxes(read_weight, 1, 2)
    state_inner, state_write, state_read = (
        jnp.swapaxes(s, 1, 2) for s in (state_inner, state_write, state_read)
    )
    recurrent = recurrent.reshape(2, 8, 128, 128)
    weights = (gate_weight, inner_weight, write_weight, read_weight, step_weight)

    first = pl.pallas_call(
        begin,
        name="begin",
        out_shape=jax.ShapeDtypeStruct((8, 128), F32),
        out_specs=pl.BlockSpec(memory_space=pltpu.VMEM),
        cost_estimate=pl.CostEstimate(flops=20000000000, bytes_accessed=0, transcendentals=0),
        compiler_params=pltpu.CompilerParams(vmem_limit_bytes=1024 * 1024),
    )()
    early, beside = call(
        spread, "spread", (((64, 16, 128), BF), ((64, 8, 128), BF)), first, write_weight, read_weight
    )
    small = (conv_inner, conv_write, conv_read, step_bias, decay_log, skip_gain, group_gain)
    small = (*small, state_inner, state_write, state_read)
    out, own, *small = call(
        lambda t, first, hidden, gain, gate, inner, write, read, step, *small: (
            *first_project(t, hidden, gain, gate, inner, write, read, step),
            *small,
        ),
        "first_project",
        (((64, 384), BF), ((8, 128), F32)) + tuple((a.shape, a.dtype) for a in small),
        beside,
        hidden,
        norm_gain,
        *weights,
        *small,
        placed=True,
    )
    conv_inner, conv_write, conv_read, step_bias, decay_log, skip_gain, group_gain = small[:7]
    state_inner, state_write, state_read = small[7:]
    got = exchange(out.reshape(8, 8, 384), DP)
    message, parts, raw0 = call(
        first_states,
        "first_states",
        (((64, 16, 128), BF), ((32, 128), F32), ((8, 384), BF)),
        got,
        conv_inner,
        conv_write,
        conv_read,
        state_inner,
        state_write,
        state_read,
        step_bias,
        decay_log,
        early,
    )
    early = exchange(message, TP)
    message, turned, updated = scan_call(
        lambda got, parts, state, skip: first_scan(got, parts, state, skip),
        "first_scan",
        (((8, 8, 128), BF), ((40, 256), F32)),
        (early, parts, skip_gain),
        recurrent,
        None,
    )
    got = exchange(message, DP)
    (out,) = call(first_finish, "first_finish", (((64, 8, 128), BF),), got, group_gain, out_weight)
    got = exchange(out, TP)
    (out,) = call(first_combine, "first_combine", (((64, 8, 128), BF),), got, own, beside)
    got = exchange(out, TP)
    out, own = call(
        second_project,
        "second_project",
        (((64, 640), BF), ((32, 128), F32)),
        got,
        norm_gain,
        *weights,
        early,
        placed=True,
    )
    got = exchange(out.reshape(8, 8, 640), DP)
    message, raw1, second, updated = scan_call(
        second_scan,
        "second_scan",
        (((8, 8, 128), BF), ((8, 640), BF)),
        (got, turned, conv_inner, state_inner, step_bias, decay_log, skip_gain),
        recurrent,
        updated,
    )
    got = exchange(message, DP)
    (out,) = call(second_finish, "second_finish", (((8, 40, 128), BF),), got, group_gain, out_weight)
    got = exchange(out, Y)
    (out,) = call(second_scale, "second_scale", (((8, 32, 128), BF),), got)
    got = exchange(out, Z)
    (out,) = call(second_combine, "second_combine", (((8, 32, 128), BF),), got, own)
    got = exchange(out, Y)
    result, next_inner, next_write, next_read, updated = last_call(
        (((64, 512), BF), ((2, 3, 8, 128), BF), ((2, 3, 8, 32), BF), ((2, 3, 8, 32), BF)),
        (got, raw0, raw1, state_inner, state_write, state_read),
        second,
        updated,
    )
    return (
        result,
        jnp.swapaxes(next_inner, 1, 2),
        jnp.swapaxes(next_write, 1, 2),
        jnp.swapaxes(next_read, 1, 2),
        updated.reshape(2, 8, 2, 64, 128),
    )


def solution(mesh):
    finer = Mesh(mesh.devices.reshape(8, 8, 4, 2), ("tp_0", "tp_1", "dp_0", "dp_1"))
    placed = (
        P(None, DP),
        P(None, DP),
        P(None, DP, TP),
        P(None, DP, TP),
        P(None, DP, TP),
        P(None, DP, TP),
        P(None, DP, None),
        P(None, None, TP),
        P(None, None, TP),
        P(None, None, TP),
        P(None, TP),
        P(None, TP),
        P(None, TP),
        P(None, TP),
        P(None, TP, DP),
        P(None, DP, None, TP),
        P(None, DP, None, TP),
        P(None, DP, None, TP),
        P(None, DP, TP, None, None),
    )
    return jax.shard_map(
        local,
        mesh=finer,
        in_specs=placed,
        out_specs=(
            P(None, DP),
            P(None, DP, None, TP),
            P(None, DP, None, TP),
            P(None, DP, None, TP),
            P(None, DP, TP, None, None),
        ),
        check_vma=False,
    )
```

```python
import jax
import jax.numpy as jnp
from jax import lax
from jax.experimental import pallas as pl
from jax.experimental.pallas import tpu as pltpu
from jax.sharding import Mesh
from jax.sharding import PartitionSpec as P

D = 4096
DP = ("dp_0", "dp_1")
TP = ("tp_0", "tp_1")
Y = "tp_1"
Z = "tp_0"
EPS = 1e-06
BF = jnp.bfloat16
F32 = jnp.float32


def iota(shape, dim):
    return lax.broadcasted_iota(jnp.int32, shape, dim)


def dot(a, b):
    return lax.dot_general(a, b, (((1,), (0,)), ((), ())), preferred_element_type=F32)


def dot_rows(a, b):
    return lax.dot_general(a, b, (((1,), (1,)), ((), ())), preferred_element_type=F32)


def silu(a):
    return a * (1.0 / (1.0 + jnp.exp(-a)))


def rounded(a):
    return a.astype(BF).astype(F32)


def one_hot(test):
    return test.astype(F32).astype(BF)


def channel(k, group):
    return k // 2 * 32 + k % 2 * 16 + group


def to_groups(entry, blocks, pick):
    width = 64 * len(blocks)
    row, col = iota((512, width), 0), iota((512, width), 1)
    here = (col % 64 == channel(entry(row % 8), row // 32)) & (col // 64 == pick(row % 8))
    return dot(one_hot(here), jnp.concatenate(blocks, axis=0))


def quarters(weights):
    return [weights[:, 128 * q : 128 * q + 128] for q in range(4)]


def from_groups(*got):
    row, col = iota((512, 512), 0), iota((512, 512), 1)
    side = jnp.concatenate([g.reshape(512, 128) for g in got], axis=1)
    return dot(one_hot(col == row % 64 * 8 + row // 64), side).astype(BF)


def side_by_side(rows, first):
    return jnp.concatenate([rows[64 * j : 64 * j + 64] for j in range(first, first + 4)], axis=1)


def spread(first, write_w, read_w):
    weights = jnp.concatenate([write_w[1], read_w[1]], axis=0)
    rolled = jnp.concatenate([weights[:, 64:], weights[:, :64]], axis=1)
    odd, even = quarters(weights), quarters(rolled)
    halves = [odd[i // 2] if i % 2 else even[(i // 2 + 3) % 4] for i in range(8)]
    early = to_groups(lambda j: j // 4, odd, lambda j: j % 4)
    late = to_groups(lambda j: 0 * j + 2, odd, lambda j: j)
    message = jnp.concatenate([m.astype(BF).reshape(64, 8, 128) for m in (early, late)], axis=1)
    beside = to_groups(lambda j: 0 * j + 3, halves, lambda j: j)
    return message, beside.astype(BF).reshape(64, 8, 128)


def project(t, wide, gain, gate_w, inner_w, write_w, read_w, step_w, extra):
    scaled = (wide * gain).astype(BF)
    squares = jnp.sum(wide * wide, axis=1, keepdims=True)
    high = rounded(squares)
    vectors = dot_rows(scaled, jnp.concatenate([write_w, read_w], axis=0))
    step = dot(scaled, step_w).astype(BF)
    row, col = iota((128, 128), 0), iota((128, 128), 1)
    mine = ((col - 64 == row - 2 * t) & (col >= 64) & (col < 66)).astype(F32).astype(BF)
    lane = iota((64, 128), 1)
    third = jnp.concatenate([vectors, jnp.zeros((64, 64), F32)], axis=1) + dot(step, mine)
    third = jnp.where(lane == 66, high, jnp.where(lane == 67, squares - high, third))
    parts = [dot(scaled, gate_w), dot(scaled, inner_w), third]
    if extra is not None:
        parts.append(dot_rows(scaled, extra))
    return jnp.concatenate(parts, axis=1).astype(BF)


def first_project(t, hidden, gain, gate_w, inner_w, write_w, read_w, step_w):
    out = project(
        t, hidden.astype(F32), gain[0:1], gate_w[0], inner_w[0], write_w[0], read_w[0], step_w[0], None
    )
    pick = (iota((8, 512), 1) == iota((8, 512), 0) + 8 * t).astype(F32).astype(BF)
    own = jnp.concatenate([dot_rows(pick, hidden), jnp.zeros((8, 64), F32)], axis=1)
    return out, own


def turned_back(got):
    return jnp.transpose(got.reshape(512, 128).astype(F32))[:64]


def second_project(t, got, gain, gate_w, inner_w, write_w, read_w, step_w, early):
    wide = turned_back(got)
    both = from_groups(early[:, :8], early[:, 8:], got)
    early, middle, late = both[:, :128], both[:, 128:256], both[:, 256:]
    blocks = [late[64 * i : 64 * i + 64] for i in range(8)]
    low = iota((64, 128), 1) < 64
    pairs = []
    for q in range(4):
        even, odd = blocks[2 * q].astype(F32), blocks[2 * q + 1].astype(F32)
        even = jnp.concatenate([even[:, 64:], even[:, :64]], axis=1)
        pairs.append(jnp.where(low, even, odd).astype(BF))
    later = jnp.concatenate(
        [
            side_by_side(early, 0),
            side_by_side(early, 4),
            side_by_side(middle, 0),
            jnp.concatenate(pairs, axis=1),
        ],
        axis=0,
    )
    out = project(t, wide, gain[1:2], gate_w[1], inner_w[1], write_w[1], read_w[1], step_w[1], later)
    row, col = iota((32, 512), 0), iota((32, 512), 1)
    first = t % 8 * 32
    rows = got.reshape(512, 128)
    own = [dot(one_hot(col == row + first + half), rows)[:, :64] for half in (0, 256)]
    return out, jnp.concatenate(own, axis=1)


def arrive(got):
    total = got[0].astype(F32)
    for k in range(1, 8):
        total = total + got[k].astype(F32)
    squares = total[:, 322:323] + total[:, 323:324]
    return (total * lax.rsqrt(squares / D + EPS)).astype(BF)


def convolve(rows, fresh, taps):
    total = fresh.astype(F32) * taps[3:4].astype(F32)
    for k in range(3):
        total = total + rows[k].astype(F32) * taps[k : k + 1].astype(F32)
    return silu(total)


def by_head(pair):
    return jnp.where(iota((8, 128), 1) < 64, pair[:, 0:1], pair[:, 1:2])


def local_parts(raw, number, conv_inner, state_inner, bias, decay):
    inner = convolve(state_inner[number], raw[:, 128:256], conv_inner[number])
    shifted = raw[:, 320:322].astype(F32) + bias[number : number + 1]
    step = jnp.maximum(shifted, 0.0) + jnp.log1p(jnp.exp(-jnp.abs(shifted)))
    retain = jnp.exp(-step * jnp.exp(decay[number : number + 1]))
    gate = silu(raw[:, :128].astype(F32))
    return inner, by_head(step), by_head(retain), gate


def next_rows(state, fresh):
    return jnp.concatenate([state[1:], fresh[None]], axis=0)


def first_states(got, conv_inner, conv_write, conv_read, state_inner, state_write, state_read, bias, decay, early):
    raw = arrive(got)
    inner, step, retain, gate = local_parts(raw, 0, conv_inner, state_inner, bias, decay)
    vec_state = jnp.concatenate([state_write, state_read], axis=3).astype(F32)
    vec_taps = jnp.concatenate([conv_write, conv_read], axis=2).astype(F32)
    acts = convolve(vec_state[0], raw[:, 256:320], vec_taps[0])
    extras = jnp.concatenate(
        [
            acts,
            vec_taps[1],
            jnp.zeros((4, 64), F32),
            vec_state[1].reshape(24, 64),
            jnp.zeros((88, 64), F32),
        ],
        axis=0,
    ).astype(BF)
    row, col = iota((512, 64), 0), iota((512, 64), 1)
    here = one_hot((row % 8 >= 4) & (col == channel(row % 8 - 4, row // 32)))
    late = dot_rows(here, extras).reshape(64, 8, 128) + early[:, 8:].astype(F32)
    message = jnp.concatenate([early[:, :8], late.astype(BF)], axis=1)
    return message, jnp.concatenate([inner, step, retain, gate], axis=0), raw


def sort_vectors(acts):
    row, col = iota((256, 256), 0), iota((256, 256), 1)
    order = one_hot(row == col // 128 * 128 + col % 2 * 64 + col % 128 // 2)
    both = dot(acts.astype(BF), order)
    return both[:, :128], both[:, 128:]


def scan_step(recurrent, inner, step, retain, gate, write_vec, read_vec, skip):
    turned = jnp.transpose(jnp.concatenate([step * inner, jnp.zeros((120, 128), F32)], axis=0))
    lane = iota((128, 128), 1)
    updated, reads = [], jnp.zeros((128, 128), F32)
    for b in range(8):
        kept = [jnp.broadcast_to(retain[b : b + 1, c : c + 1], (64, 128)) for c in (0, 64)]
        new = jnp.concatenate(kept, axis=0) * recurrent[b] + turned[:, b : b + 1] * write_vec[b : b + 1]
        updated.append(new)
        reads = jnp.where(lane == b, jnp.sum(new * read_vec[b : b + 1], axis=1, keepdims=True), reads)
    readout = jnp.transpose(reads)[:8] + by_head(jnp.broadcast_to(skip, (8, 2))) * inner
    gated = (readout * gate).astype(BF)
    return updated, jnp.broadcast_to(gated[None], (8, 8, 128))


def first_scan(got, parts, recurrent, skip):
    row, col = iota((256, 512), 0), iota((256, 512), 1)
    extras = dot(one_hot(col == row % 64 * 8 + 4 + row // 64), got[:, 8:].reshape(512, 128))
    turned = jnp.transpose(extras)[:40]
    write_vec, read_vec = sort_vectors(turned[:8])
    updated, message = scan_step(
        recurrent[0], parts[:8], parts[8:16], parts[16:24], parts[24:], write_vec, read_vec, skip[0:1]
    )
    return message, turned, updated


def second_scan(got, turned, conv_inner, state_inner, bias, decay, recurrent, skip):
    raw = arrive(got)
    inner, step, retain, gate = local_parts(raw, 1, conv_inner, state_inner, bias, decay)
    rows = turned[16:40].reshape(3, 8, 256)
    acts = convolve(rows, raw[:, 384:], turned[8:12])
    write_vec, read_vec = sort_vectors(acts)
    updated, message = scan_step(recurrent[1], inner, step, retain, gate, write_vec, read_vec, skip[1:2])
    return message, raw, updated


def partial(number, got, gain, out_w):
    wide = got.reshape(64, 128).astype(F32)
    squares = jnp.sum(wide * wide, axis=1, keepdims=True)
    part = dot((wide * gain[number : number + 1]).astype(BF), out_w[number])
    return jnp.transpose(jnp.concatenate([part, jnp.broadcast_to(squares, (64, 512))], axis=0))


def first_finish(got, gain, out_w):
    turned = partial(0, got, gain, out_w)
    high = rounded(turned)
    lane, row = iota((512, 128), 1), iota((512, 128), 0)
    out = jnp.where((lane < 64) | (row % 8 < 4), turned, turned - high).astype(BF)
    return (out.reshape(64, 8, 128),)


def first_combine(got, own, beside):
    some = got.astype(F32).reshape(16, 4, 8, 128)
    some = some[:, 0] + some[:, 1] + some[:, 2] + some[:, 3]
    both = some + jnp.concatenate([some[:, 4:], some[:, :4]], axis=1)
    factor = lax.rsqrt(both / 512 + EPS)
    factor = jnp.concatenate([factor[:, :, 64:], factor[:, :, :64]], axis=2)
    new = own + jnp.sum(some * factor, axis=0)
    low = iota((64, 8, 128), 2) < 64
    return (jnp.where(low, jnp.broadcast_to(new[None], (64, 8, 128)), beside.astype(F32)).astype(BF),)


def second_finish(got, gain, out_w):
    turned = partial(1, got, gain, out_w)
    out = jnp.concatenate([turned[:256, :64], turned[256:, :64]], axis=1)
    squares = jnp.concatenate([turned[:8, 64:], turned[:8, 64:]], axis=1)
    high = rounded(squares)
    squares = jnp.where(iota((8, 128), 0) < 4, high, squares - high)
    squares = jnp.broadcast_to(squares[None], (8, 8, 128))
    return (jnp.concatenate([out.reshape(8, 32, 128), squares], axis=1).astype(BF),)


def second_scale(got):
    total = jnp.zeros((32, 128), F32)
    for half in (0, 4):
        some = got[half].astype(F32)
        for k in range(1, 4):
            some = some + got[half + k].astype(F32)
        squares = some[32:33] + some[36:37]
        total = total + some[:32] * lax.rsqrt(squares / 512 + EPS)
    return (jnp.broadcast_to(total.astype(BF)[None], (8, 32, 128)),)


def second_combine(got, own):
    for k in range(8):
        own = own + got[k].astype(F32)
    return (jnp.broadcast_to(own.astype(BF)[None], (8, 32, 128)),)


def last(got, raw0, raw1, state_inner, state_write, state_read):
    turned = jnp.transpose(got.reshape(256, 128).astype(F32))
    outs = [jnp.concatenate([turned[:64], turned[64:]], axis=1).astype(BF)]
    for state, low, high in ((state_inner, 128, 256), (state_write, 256, 288), (state_read, 288, 320)):
        rows = [next_rows(state[0], raw0[:, low:high])[None], next_rows(state[1], raw1[:, low:high])[None]]
        outs.append(jnp.concatenate(rows, axis=0))
    return tuple(outs)


def call(fn, name, outs, *args, placed=False):
    n_in = len(args)

    def kernel(*refs):
        values = [r[...] for r in refs[:n_in]]
        dest = refs[n_in:]
        if placed:
            values = [lax.axis_index(Z) * 8 + lax.axis_index(Y)] + values
        for ref, value in zip(dest, fn(*values)):
            ref[...] = value

    whole = pl.BlockSpec(memory_space=pltpu.VMEM)
    specs = [whole] * n_in
    return pl.pallas_call(
        kernel,
        name=name,
        out_shape=tuple(jax.ShapeDtypeStruct(s, d) for s, d in outs),
        in_specs=specs,
        out_specs=tuple(whole for _ in outs),
        compiler_params=pltpu.CompilerParams(vmem_limit_bytes=16 * 1024 * 1024),
    )(*args)


def begin(out_ref):
    out_ref[...] = jnp.zeros((8, 128), F32)


def start_copies(source, dest, sems):
    copies = [pltpu.make_async_copy(source.at[b], dest.at[b], sems.at[b]) for b in range(8)]
    for copy in copies:
        copy.start()
    return copies


def scan_call(fn, name, outs, args, recurrent, earlier):
    n_in = len(args)

    def kernel(*refs):
        values = [r[...] for r in refs[:n_in]]
        state = refs[n_in]
        if earlier is None:
            dest = refs[n_in + 1 :]
        else:
            dest, whole_ref, sem = refs[n_in + 2 : -2], refs[-2], refs[-1]
            copies = start_copies(refs[n_in + 1], whole_ref.at[0], sem)
        results = fn(*values[:-1], state, values[-1])
        for ref, value in zip(dest[:-1], results[:-1]):
            ref[...] = value
        for b in range(8):
            dest[-1][b] = results[-1][b]
        if earlier is not None:
            for copy in copies:
                copy.wait()

    whole = pl.BlockSpec(memory_space=pltpu.VMEM)
    specs = [whole] * (n_in + 1 + (earlier is not None))
    operands = (*args, recurrent) + (() if earlier is None else (earlier,))
    outs = (*outs, ((8, 128, 128), F32))
    out_specs = [whole] * len(outs)
    if earlier is not None:
        outs = (*outs, ((2, 8, 128, 128), F32))
        out_specs.append(pl.BlockSpec(memory_space=pl.ANY))
    return pl.pallas_call(
        kernel,
        name=name,
        out_shape=tuple(jax.ShapeDtypeStruct(s, d) for s, d in outs),
        in_specs=specs,
        out_specs=tuple(out_specs),
        scratch_shapes=[] if earlier is None else [pltpu.SemaphoreType.DMA((8,))],
        compiler_params=pltpu.CompilerParams(vmem_limit_bytes=16 * 1024 * 1024),
    )(*operands)


def last_call(outs, args, state, whole_state):
    n_in = len(args)

    def kernel(*refs):
        state_ref, dest, whole_ref, sem = refs[n_in], refs[n_in + 2 : -2], refs[-2], refs[-1]
        copies = start_copies(state_ref, whole_ref.at[1], sem)
        for ref, value in zip(dest, last(*[r[...] for r in refs[:n_in]])):
            ref[...] = value
        for copy in copies:
            copy.wait()

    whole, anywhere = pl.BlockSpec(memory_space=pltpu.VMEM), pl.BlockSpec(memory_space=pl.ANY)
    return pl.pallas_call(
        kernel,
        name="last",
        out_shape=tuple(jax.ShapeDtypeStruct(s, d) for s, d in outs)
        + (jax.ShapeDtypeStruct(whole_state.shape, F32),),
        in_specs=[whole] * (n_in + 1) + [anywhere],
        out_specs=tuple(whole for _ in outs) + (anywhere,),
        input_output_aliases={n_in + 1: len(outs)},
        scratch_shapes=[pltpu.SemaphoreType.DMA((8,))],
        compiler_params=pltpu.CompilerParams(vmem_limit_bytes=16 * 1024 * 1024),
    )(*args, state, whole_state)


def exchange(pieces, axis):
    return lax.all_to_all(pieces, axis, 0, 0, tiled=True)


def local(
    hidden,
    norm_gain,
    gate_weight,
    inner_weight,
    write_weight,
    read_weight,
    step_weight,
    conv_inner,
    conv_write,
    conv_read,
    step_bias,
    decay_log,
    skip_gain,
    group_gain,
    out_weight,
    state_inner,
    state_write,
    state_read,
    recurrent,
):
    write_weight, read_weight = jnp.swapaxes(write_weight, 1, 2), jnp.swapaxes(read_weight, 1, 2)
    state_inner, state_write, state_read = (
        jnp.swapaxes(s, 1, 2) for s in (state_inner, state_write, state_read)
    )
    recurrent = recurrent.reshape(2, 8, 128, 128)
    weights = (gate_weight, inner_weight, write_weight, read_weight, step_weight)

    first = pl.pallas_call(
        begin,
        name="begin",
        out_shape=jax.ShapeDtypeStruct((8, 128), F32),
        out_specs=pl.BlockSpec(memory_space=pltpu.VMEM),
        cost_estimate=pl.CostEstimate(flops=20000000000, bytes_accessed=0, transcendentals=0),
        compiler_params=pltpu.CompilerParams(vmem_limit_bytes=1024 * 1024),
    )()
    small = (conv_inner, conv_write, conv_read, step_bias, decay_log, skip_gain, group_gain)
    small = (*small, state_inner, state_write, state_read, norm_gain)
    early, beside, *small = call(
        lambda first, write, read, *small: (*spread(first, write, read), *small),
        "spread",
        (((64, 16, 128), BF), ((64, 8, 128), BF)) + tuple((a.shape, a.dtype) for a in small),
        first,
        write_weight,
        read_weight,
        *small,
    )
    norm_gain = small[10]
    out, own = call(
        lambda t, beside, *rest: first_project(t, *rest),
        "first_project",
        (((64, 384), BF), ((8, 128), F32)),
        beside,
        hidden,
        norm_gain,
        *weights,
        placed=True,
    )
    conv_inner, conv_write, conv_read, step_bias, decay_log, skip_gain, group_gain = small[:7]
    state_inner, state_write, state_read = small[7:10]
    got = exchange(out.reshape(8, 8, 384), DP)
    message, parts, raw0 = call(
        first_states,
        "first_states",
        (((64, 16, 128), BF), ((32, 128), F32), ((8, 384), BF)),
        got,
        conv_inner,
        conv_write,
        conv_read,
        state_inner,
        state_write,
        state_read,
        step_bias,
        decay_log,
        early,
    )
    early = exchange(message, TP)
    message, turned, updated = scan_call(
        lambda got, parts, state, skip: first_scan(got, parts, state, skip),
        "first_scan",
        (((8, 8, 128), BF), ((40, 256), F32)),
        (early, parts, skip_gain),
        recurrent,
        None,
    )
    got = exchange(message, DP)
    (out,) = call(first_finish, "first_finish", (((64, 8, 128), BF),), got, group_gain, out_weight)
    got = exchange(out, TP)
    (out,) = call(first_combine, "first_combine", (((64, 8, 128), BF),), got, own, beside)
    got = exchange(out, TP)
    out, own = call(
        second_project,
        "second_project",
        (((64, 640), BF), ((32, 128), F32)),
        got,
        norm_gain,
        *weights,
        early,
        placed=True,
    )
    got = exchange(out.reshape(8, 8, 640), DP)
    message, raw1, second, updated = scan_call(
        second_scan,
        "second_scan",
        (((8, 8, 128), BF), ((8, 640), BF)),
        (got, turned, conv_inner, state_inner, step_bias, decay_log, skip_gain),
        recurrent,
        updated,
    )
    got = exchange(message, DP)
    (out,) = call(second_finish, "second_finish", (((8, 40, 128), BF),), got, group_gain, out_weight)
    got = exchange(out, Y)
    (out,) = call(second_scale, "second_scale", (((8, 32, 128), BF),), got)
    got = exchange(out, Z)
    (out,) = call(second_combine, "second_combine", (((8, 32, 128), BF),), got, own)
    got = exchange(out, Y)
    result, next_inner, next_write, next_read, updated = last_call(
        (((64, 512), BF), ((2, 3, 8, 128), BF), ((2, 3, 8, 32), BF), ((2, 3, 8, 32), BF)),
        (got, raw0, raw1, state_inner, state_write, state_read),
        second,
        updated,
    )
    return (
        result,
        jnp.swapaxes(next_inner, 1, 2),
        jnp.swapaxes(next_write, 1, 2),
        jnp.swapaxes(next_read, 1, 2),
        updated.reshape(2, 8, 2, 64, 128),
    )


def solution(mesh):
    finer = Mesh(mesh.devices.reshape(8, 8, 4, 2), ("tp_0", "tp_1", "dp_0", "dp_1"))
    placed = (
        P(None, DP),
        P(None, DP),
        P(None, DP, TP),
        P(None, DP, TP),
        P(None, DP, TP),
        P(None, DP, TP),
        P(None, DP, None),
        P(None, None, TP),
        P(None, None, TP),
        P(None, None, TP),
        P(None, TP),
        P(None, TP),
        P(None, TP),
        P(None, TP),
        P(None, TP, DP),
        P(None, DP, None, TP),
        P(None, DP, None, TP),
        P(None, DP, None, TP),
        P(None, DP, TP, None, None),
    )
    return jax.shard_map(
        local,
        mesh=finer,
        in_specs=placed,
        out_specs=(
            P(None, DP),
            P(None, DP, None, TP),
            P(None, DP, None, TP),
            P(None, DP, None, TP),
            P(None, DP, TP, None, None),
        ),
        check_vma=False,
    )
```

```python
import jax
import jax.numpy as jnp
from jax import lax
from jax.experimental import pallas as pl
from jax.experimental.pallas import tpu as pltpu
from jax.sharding import Mesh
from jax.sharding import PartitionSpec as P

D = 4096
DP = ("dp_0", "dp_1")
TP = ("tp_0", "tp_1")
Y = "tp_1"
Z = "tp_0"
EPS = 1e-06
BF = jnp.bfloat16
F32 = jnp.float32


def iota(shape, dim):
    return lax.broadcasted_iota(jnp.int32, shape, dim)


def dot(a, b):
    return lax.dot_general(a, b, (((1,), (0,)), ((), ())), preferred_element_type=F32)


def dot_rows(a, b):
    return lax.dot_general(a, b, (((1,), (1,)), ((), ())), preferred_element_type=F32)


def silu(a):
    return a * (1.0 / (1.0 + jnp.exp(-a)))


def rounded(a):
    return a.astype(BF).astype(F32)


def one_hot(test):
    return test.astype(F32).astype(BF)


def channel(k, group):
    return k // 2 * 32 + k % 2 * 16 + group


def to_groups(entry, blocks, pick):
    width = 64 * len(blocks)
    row, col = iota((512, width), 0), iota((512, width), 1)
    here = (col % 64 == channel(entry(row % 8), row // 32)) & (col // 64 == pick(row % 8))
    return dot(one_hot(here), jnp.concatenate(blocks, axis=0))


def quarters(weights):
    return [weights[:, 128 * q : 128 * q + 128] for q in range(4)]


def from_groups(*got):
    row, col = iota((512, 512), 0), iota((512, 512), 1)
    side = jnp.concatenate([g.reshape(512, 128) for g in got], axis=1)
    return dot(one_hot(col == row % 64 * 8 + row // 64), side).astype(BF)


def side_by_side(rows, first):
    return jnp.concatenate([rows[64 * j : 64 * j + 64] for j in range(first, first + 4)], axis=1)


def spread(first, write_w, read_w):
    weights = jnp.concatenate([write_w[1], read_w[1]], axis=0)
    rolled = jnp.concatenate([weights[:, 64:], weights[:, :64]], axis=1)
    odd, even = quarters(weights), quarters(rolled)
    halves = [odd[i // 2] if i % 2 else even[(i // 2 + 3) % 4] for i in range(8)]
    early = to_groups(lambda j: j // 4, odd, lambda j: j % 4)
    late = to_groups(lambda j: 0 * j + 2, odd, lambda j: j)
    message = jnp.concatenate([m.astype(BF).reshape(64, 8, 128) for m in (early, late)], axis=1)
    beside = to_groups(lambda j: 0 * j + 3, halves, lambda j: j)
    return message, beside.astype(BF).reshape(64, 8, 128)


def project(t, wide, gain, gate_w, inner_w, write_w, read_w, step_w, extra):
    scaled = (wide * gain).astype(BF)
    squares = jnp.sum(wide * wide, axis=1, keepdims=True)
    high = rounded(squares)
    vectors = dot_rows(scaled, jnp.concatenate([write_w, read_w], axis=0))
    step = dot(scaled, step_w).astype(BF)
    row, col = iota((128, 128), 0), iota((128, 128), 1)
    mine = ((col - 64 == row - 2 * t) & (col >= 64) & (col < 66)).astype(F32).astype(BF)
    lane = iota((64, 128), 1)
    third = jnp.concatenate([vectors, jnp.zeros((64, 64), F32)], axis=1) + dot(step, mine)
    third = jnp.where(lane == 66, high, jnp.where(lane == 67, squares - high, third))
    parts = [dot(scaled, gate_w), dot(scaled, inner_w), third]
    if extra is not None:
        parts.append(dot_rows(scaled, extra))
    return jnp.concatenate(parts, axis=1).astype(BF)


def first_project(t, hidden, gain, gate_w, inner_w, write_w, read_w, step_w):
    out = project(
        t, hidden.astype(F32), gain[0:1], gate_w[0], inner_w[0], write_w[0], read_w[0], step_w[0], None
    )
    pick = (iota((8, 512), 1) == iota((8, 512), 0) + 8 * t).astype(F32).astype(BF)
    own = jnp.concatenate([dot_rows(pick, hidden), jnp.zeros((8, 64), F32)], axis=1)
    return out, own


def turned_back(got):
    return jnp.transpose(got.reshape(512, 128).astype(F32))[:64]


def second_project(t, got, gain, gate_w, inner_w, write_w, read_w, step_w, early):
    wide = turned_back(got)
    both = from_groups(early[:, :8], early[:, 8:], got)
    early, middle, late = both[:, :128], both[:, 128:256], both[:, 256:]
    blocks = [late[64 * i : 64 * i + 64] for i in range(8)]
    low = iota((64, 128), 1) < 64
    pairs = []
    for q in range(4):
        even, odd = blocks[2 * q].astype(F32), blocks[2 * q + 1].astype(F32)
        even = jnp.concatenate([even[:, 64:], even[:, :64]], axis=1)
        pairs.append(jnp.where(low, even, odd).astype(BF))
    later = jnp.concatenate(
        [
            side_by_side(early, 0),
            side_by_side(early, 4),
            side_by_side(middle, 0),
            jnp.concatenate(pairs, axis=1),
        ],
        axis=0,
    )
    out = project(t, wide, gain[1:2], gate_w[1], inner_w[1], write_w[1], read_w[1], step_w[1], later)
    row, col = iota((32, 512), 0), iota((32, 512), 1)
    first = t % 8 * 32
    rows = got.reshape(512, 128)
    own = [dot(one_hot(col == row + first + half), rows)[:, :64] for half in (0, 256)]
    return out, jnp.concatenate(own, axis=1)


def arrive(got):
    total = got[0].astype(F32)
    for k in range(1, 8):
        total = total + got[k].astype(F32)
    squares = total[:, 322:323] + total[:, 323:324]
    return (total * lax.rsqrt(squares / D + EPS)).astype(BF)


def convolve(rows, fresh, taps):
    total = fresh.astype(F32) * taps[3:4].astype(F32)
    for k in range(3):
        total = total + rows[k].astype(F32) * taps[k : k + 1].astype(F32)
    return silu(total)


def by_head(pair):
    return jnp.where(iota((8, 128), 1) < 64, pair[:, 0:1], pair[:, 1:2])


def local_parts(raw, number, conv_inner, state_inner, bias, decay):
    inner = convolve(state_inner[number], raw[:, 128:256], conv_inner[number])
    shifted = raw[:, 320:322].astype(F32) + bias[number : number + 1]
    step = jnp.maximum(shifted, 0.0) + jnp.log1p(jnp.exp(-jnp.abs(shifted)))
    retain = jnp.exp(-step * jnp.exp(decay[number : number + 1]))
    gate = silu(raw[:, :128].astype(F32))
    return inner, by_head(step), by_head(retain), gate


def next_rows(state, fresh):
    return jnp.concatenate([state[1:], fresh[None]], axis=0)


def first_states(got, conv_inner, conv_write, conv_read, state_inner, state_write, state_read, bias, decay, early):
    raw = arrive(got)
    inner, step, retain, gate = local_parts(raw, 0, conv_inner, state_inner, bias, decay)
    vec_state = jnp.concatenate([state_write, state_read], axis=3).astype(F32)
    vec_taps = jnp.concatenate([conv_write, conv_read], axis=2).astype(F32)
    acts = convolve(vec_state[0], raw[:, 256:320], vec_taps[0])
    extras = jnp.concatenate(
        [
            acts,
            vec_taps[1],
            jnp.zeros((4, 64), F32),
            vec_state[1].reshape(24, 64),
            jnp.zeros((88, 64), F32),
        ],
        axis=0,
    ).astype(BF)
    row, col = iota((512, 64), 0), iota((512, 64), 1)
    here = one_hot((row % 8 >= 4) & (col == channel(row % 8 - 4, row // 32)))
    late = dot_rows(here, extras).reshape(64, 8, 128) + early[:, 8:].astype(F32)
    message = jnp.concatenate([early[:, :8], late.astype(BF)], axis=1)
    return message, jnp.concatenate([inner, step, retain, gate], axis=0), raw


def sort_vectors(acts):
    row, col = iota((256, 256), 0), iota((256, 256), 1)
    order = one_hot(row == col // 128 * 128 + col % 2 * 64 + col % 128 // 2)
    both = dot(acts.astype(BF), order)
    return both[:, :128], both[:, 128:]


def scan_step(recurrent, inner, step, retain, gate, write_vec, read_vec, skip):
    turned = jnp.transpose(jnp.concatenate([step * inner, jnp.zeros((120, 128), F32)], axis=0))
    lane = iota((128, 128), 1)
    updated, reads = [], jnp.zeros((128, 128), F32)
    for b in range(8):
        kept = [jnp.broadcast_to(retain[b : b + 1, c : c + 1], (64, 128)) for c in (0, 64)]
        new = jnp.concatenate(kept, axis=0) * recurrent[b] + turned[:, b : b + 1] * write_vec[b : b + 1]
        updated.append(new)
        reads = jnp.where(lane == b, jnp.sum(new * read_vec[b : b + 1], axis=1, keepdims=True), reads)
    readout = jnp.transpose(reads)[:8] + by_head(jnp.broadcast_to(skip, (8, 2))) * inner
    gated = (readout * gate).astype(BF)
    return updated, jnp.broadcast_to(gated[None], (8, 8, 128))


def first_scan(got, parts, recurrent, skip):
    row, col = iota((256, 512), 0), iota((256, 512), 1)
    extras = dot(one_hot(col == row % 64 * 8 + 4 + row // 64), got[:, 8:].reshape(512, 128))
    turned = jnp.transpose(extras)[:40]
    write_vec, read_vec = sort_vectors(turned[:8])
    updated, message = scan_step(
        recurrent[0], parts[:8], parts[8:16], parts[16:24], parts[24:], write_vec, read_vec, skip[0:1]
    )
    return message, turned, updated


def second_scan(got, turned, conv_inner, state_inner, bias, decay, recurrent, skip):
    raw = arrive(got)
    inner, step, retain, gate = local_parts(raw, 1, conv_inner, state_inner, bias, decay)
    rows = turned[16:40].reshape(3, 8, 256)
    acts = convolve(rows, raw[:, 384:], turned[8:12])
    write_vec, read_vec = sort_vectors(acts)
    updated, message = scan_step(recurrent[1], inner, step, retain, gate, write_vec, read_vec, skip[1:2])
    return message, raw, updated


def partial(number, got, gain, out_w):
    wide = got.reshape(64, 128).astype(F32)
    squares = jnp.sum(wide * wide, axis=1, keepdims=True)
    part = dot((wide * gain[number : number + 1]).astype(BF), out_w[number])
    return jnp.transpose(jnp.concatenate([part, jnp.broadcast_to(squares, (64, 512))], axis=0))


def first_finish(got, gain, out_w):
    turned = partial(0, got, gain, out_w)
    high = rounded(turned)
    lane, row = iota((512, 128), 1), iota((512, 128), 0)
    out = jnp.where((lane < 64) | (row % 8 < 4), turned, turned - high).astype(BF)
    return (out.reshape(64, 8, 128),)


def first_combine(got, own, beside):
    some = got.astype(F32).reshape(16, 4, 8, 128)
    some = some[:, 0] + some[:, 1] + some[:, 2] + some[:, 3]
    both = some + jnp.concatenate([some[:, 4:], some[:, :4]], axis=1)
    factor = lax.rsqrt(both / 512 + EPS)
    factor = jnp.concatenate([factor[:, :, 64:], factor[:, :, :64]], axis=2)
    new = own + jnp.sum(some * factor, axis=0)
    low = iota((64, 8, 128), 2) < 64
    return (jnp.where(low, jnp.broadcast_to(new[None], (64, 8, 128)), beside.astype(F32)).astype(BF),)


def second_finish(got, gain, out_w):
    turned = partial(1, got, gain, out_w)
    out = jnp.concatenate([turned[:256, :64], turned[256:, :64]], axis=1)
    squares = jnp.concatenate([turned[:8, 64:], turned[:8, 64:]], axis=1)
    high = rounded(squares)
    squares = jnp.where(iota((8, 128), 0) < 4, high, squares - high)
    squares = jnp.broadcast_to(squares[None], (8, 8, 128))
    return (jnp.concatenate([out.reshape(8, 32, 128), squares], axis=1).astype(BF),)


def second_scale(got):
    total = jnp.zeros((32, 128), F32)
    for half in (0, 4):
        some = got[half].astype(F32)
        for k in range(1, 4):
            some = some + got[half + k].astype(F32)
        squares = some[32:33] + some[36:37]
        total = total + some[:32] * lax.rsqrt(squares / 512 + EPS)
    return (jnp.broadcast_to(total.astype(BF)[None], (8, 32, 128)),)


def second_combine(got, own):
    for k in range(8):
        own = own + got[k].astype(F32)
    return (jnp.broadcast_to(own.astype(BF)[None], (8, 32, 128)),)


def last(got, raw0, raw1, state_inner, state_write, state_read):
    turned = jnp.transpose(got.reshape(256, 128).astype(F32))
    outs = [jnp.concatenate([turned[:64], turned[64:]], axis=1).astype(BF)]
    for state, low, high in ((state_inner, 128, 256), (state_write, 256, 288), (state_read, 288, 320)):
        rows = [next_rows(state[0], raw0[:, low:high])[None], next_rows(state[1], raw1[:, low:high])[None]]
        outs.append(jnp.concatenate(rows, axis=0))
    return tuple(outs)


def call(fn, name, outs, *args, placed=False):
    n_in = len(args)

    def kernel(*refs):
        values = [r[...] for r in refs[:n_in]]
        dest = refs[n_in:]
        if placed:
            values = [lax.axis_index(Z) * 8 + lax.axis_index(Y)] + values
        for ref, value in zip(dest, fn(*values)):
            ref[...] = value

    whole = pl.BlockSpec(memory_space=pltpu.VMEM)
    specs = [whole] * n_in
    return pl.pallas_call(
        kernel,
        name=name,
        out_shape=tuple(jax.ShapeDtypeStruct(s, d) for s, d in outs),
        in_specs=specs,
        out_specs=tuple(whole for _ in outs),
        compiler_params=pltpu.CompilerParams(vmem_limit_bytes=16 * 1024 * 1024),
    )(*args)


def begin(out_ref):
    out_ref[...] = jnp.zeros((8, 128), F32)


def start_copies(source, dest, sems, rows=range(8)):
    copies = [pltpu.make_async_copy(source.at[b], dest.at[b], sems.at[b]) for b in rows]
    for copy in copies:
        copy.start()
    return copies


def scan_call(fn, name, outs, args, recurrent, earlier):
    n_in = len(args)

    def kernel(*refs):
        values = [r[...] for r in refs[:n_in]]
        state = refs[n_in]
        if earlier is None:
            dest = refs[n_in + 1 :]
        else:
            dest, whole_ref, sem = refs[n_in + 3 : -2], refs[-2], refs[-1]
            copies = start_copies(refs[n_in + 1], whole_ref.at[0], sem, range(4, 8))
        results = fn(*values[:-1], state, values[-1])
        for ref, value in zip(dest[:-1], results[:-1]):
            ref[...] = value
        for b in range(8):
            dest[-1][b] = results[-1][b]
        if earlier is not None:
            for copy in copies:
                copy.wait()

    whole = pl.BlockSpec(memory_space=pltpu.VMEM)
    specs = [whole] * (n_in + 1)
    operands = (*args, recurrent)
    if earlier is not None:
        specs += [whole, pl.BlockSpec(memory_space=pl.ANY)]
        operands += earlier
    outs = (*outs, ((8, 128, 128), F32))
    out_specs = [whole] * len(outs)
    if earlier is not None:
        outs = (*outs, ((2, 8, 128, 128), F32))
        out_specs.append(pl.BlockSpec(memory_space=pl.ANY))
    return pl.pallas_call(
        kernel,
        name=name,
        out_shape=tuple(jax.ShapeDtypeStruct(s, d) for s, d in outs),
        in_specs=specs,
        out_specs=tuple(out_specs),
        input_output_aliases={} if earlier is None else {n_in + 2: len(outs) - 1},
        scratch_shapes=[] if earlier is None else [pltpu.SemaphoreType.DMA((8,))],
        compiler_params=pltpu.CompilerParams(vmem_limit_bytes=16 * 1024 * 1024),
    )(*operands)


def second_project_call(outs, args, state):
    n_in = len(args)

    def kernel(*refs):
        dest, whole_ref, sem = refs[n_in + 1 : -2], refs[-2], refs[-1]
        copies = start_copies(refs[n_in], whole_ref.at[0], sem, range(4))
        t = lax.axis_index(Z) * 8 + lax.axis_index(Y)
        for ref, value in zip(dest, second_project(t, *[r[...] for r in refs[:n_in]])):
            ref[...] = value
        for copy in copies:
            copy.wait()

    whole = pl.BlockSpec(memory_space=pltpu.VMEM)
    return pl.pallas_call(
        kernel,
        name="second_project",
        out_shape=tuple(jax.ShapeDtypeStruct(s, d) for s, d in outs)
        + (jax.ShapeDtypeStruct((2, 8, 128, 128), F32),),
        in_specs=[whole] * (n_in + 1),
        out_specs=tuple(whole for _ in outs) + (pl.BlockSpec(memory_space=pl.ANY),),
        scratch_shapes=[pltpu.SemaphoreType.DMA((8,))],
        compiler_params=pltpu.CompilerParams(vmem_limit_bytes=16 * 1024 * 1024),
    )(*args, state)


def last_call(outs, args, state, whole_state):
    n_in = len(args)

    def kernel(*refs):
        state_ref, dest, whole_ref, sem = refs[n_in], refs[n_in + 2 : -2], refs[-2], refs[-1]
        copies = start_copies(state_ref, whole_ref.at[1], sem)
        for ref, value in zip(dest, last(*[r[...] for r in refs[:n_in]])):
            ref[...] = value
        for copy in copies:
            copy.wait()

    whole, anywhere = pl.BlockSpec(memory_space=pltpu.VMEM), pl.BlockSpec(memory_space=pl.ANY)
    return pl.pallas_call(
        kernel,
        name="last",
        out_shape=tuple(jax.ShapeDtypeStruct(s, d) for s, d in outs)
        + (jax.ShapeDtypeStruct(whole_state.shape, F32),),
        in_specs=[whole] * (n_in + 1) + [anywhere],
        out_specs=tuple(whole for _ in outs) + (anywhere,),
        input_output_aliases={n_in + 1: len(outs)},
        scratch_shapes=[pltpu.SemaphoreType.DMA((8,))],
        compiler_params=pltpu.CompilerParams(vmem_limit_bytes=16 * 1024 * 1024),
    )(*args, state, whole_state)


def exchange(pieces, axis):
    return lax.all_to_all(pieces, axis, 0, 0, tiled=True)


def local(
    hidden,
    norm_gain,
    gate_weight,
    inner_weight,
    write_weight,
    read_weight,
    step_weight,
    conv_inner,
    conv_write,
    conv_read,
    step_bias,
    decay_log,
    skip_gain,
    group_gain,
    out_weight,
    state_inner,
    state_write,
    state_read,
    recurrent,
):
    write_weight, read_weight = jnp.swapaxes(write_weight, 1, 2), jnp.swapaxes(read_weight, 1, 2)
    state_inner, state_write, state_read = (
        jnp.swapaxes(s, 1, 2) for s in (state_inner, state_write, state_read)
    )
    recurrent = recurrent.reshape(2, 8, 128, 128)
    weights = (gate_weight, inner_weight, write_weight, read_weight, step_weight)

    first = pl.pallas_call(
        begin,
        name="begin",
        out_shape=jax.ShapeDtypeStruct((8, 128), F32),
        out_specs=pl.BlockSpec(memory_space=pltpu.VMEM),
        cost_estimate=pl.CostEstimate(flops=20000000000, bytes_accessed=0, transcendentals=0),
        compiler_params=pltpu.CompilerParams(vmem_limit_bytes=1024 * 1024),
    )()
    small = (conv_inner, conv_write, conv_read, step_bias, decay_log, skip_gain, group_gain)
    small = (*small, state_inner, state_write, state_read, norm_gain)
    early, beside, *small = call(
        lambda first, write, read, *small: (*spread(first, write, read), *small),
        "spread",
        (((64, 16, 128), BF), ((64, 8, 128), BF)) + tuple((a.shape, a.dtype) for a in small),
        first,
        write_weight,
        read_weight,
        *small,
    )
    norm_gain = small[10]
    out, own = call(
        lambda t, beside, *rest: first_project(t, *rest),
        "first_project",
        (((64, 384), BF), ((8, 128), F32)),
        beside,
        hidden,
        norm_gain,
        *weights,
        placed=True,
    )
    conv_inner, conv_write, conv_read, step_bias, decay_log, skip_gain, group_gain = small[:7]
    state_inner, state_write, state_read = small[7:10]
    got = exchange(out.reshape(8, 8, 384), DP)
    message, parts, raw0 = call(
        first_states,
        "first_states",
        (((64, 16, 128), BF), ((32, 128), F32), ((8, 384), BF)),
        got,
        conv_inner,
        conv_write,
        conv_read,
        state_inner,
        state_write,
        state_read,
        step_bias,
        decay_log,
        early,
    )
    early = exchange(message, TP)
    message, turned, updated = scan_call(
        lambda got, parts, state, skip: first_scan(got, parts, state, skip),
        "first_scan",
        (((8, 8, 128), BF), ((40, 256), F32)),
        (early, parts, skip_gain),
        recurrent,
        None,
    )
    got = exchange(message, DP)
    (out,) = call(first_finish, "first_finish", (((64, 8, 128), BF),), got, group_gain, out_weight)
    got = exchange(out, TP)
    (out,) = call(first_combine, "first_combine", (((64, 8, 128), BF),), got, own, beside)
    got = exchange(out, TP)
    out, own, whole_state = second_project_call(
        (((64, 640), BF), ((32, 128), F32)), (got, norm_gain, *weights, early), updated
    )
    got = exchange(out.reshape(8, 8, 640), DP)
    message, raw1, second, updated = scan_call(
        second_scan,
        "second_scan",
        (((8, 8, 128), BF), ((8, 640), BF)),
        (got, turned, conv_inner, state_inner, step_bias, decay_log, skip_gain),
        recurrent,
        (updated, whole_state),
    )
    got = exchange(message, DP)
    (out,) = call(second_finish, "second_finish", (((8, 40, 128), BF),), got, group_gain, out_weight)
    got = exchange(out, Y)
    (out,) = call(second_scale, "second_scale", (((8, 32, 128), BF),), got)
    got = exchange(out, Z)
    (out,) = call(second_combine, "second_combine", (((8, 32, 128), BF),), got, own)
    got = exchange(out, Y)
    result, next_inner, next_write, next_read, updated = last_call(
        (((64, 512), BF), ((2, 3, 8, 128), BF), ((2, 3, 8, 32), BF), ((2, 3, 8, 32), BF)),
        (got, raw0, raw1, state_inner, state_write, state_read),
        second,
        updated,
    )
    return (
        result,
        jnp.swapaxes(next_inner, 1, 2),
        jnp.swapaxes(next_write, 1, 2),
        jnp.swapaxes(next_read, 1, 2),
        updated.reshape(2, 8, 2, 64, 128),
    )


def solution(mesh):
    finer = Mesh(mesh.devices.reshape(8, 8, 4, 2), ("tp_0", "tp_1", "dp_0", "dp_1"))
    placed = (
        P(None, DP),
        P(None, DP),
        P(None, DP, TP),
        P(None, DP, TP),
        P(None, DP, TP),
        P(None, DP, TP),
        P(None, DP, None),
        P(None, None, TP),
        P(None, None, TP),
        P(None, None, TP),
        P(None, TP),
        P(None, TP),
        P(None, TP),
        P(None, TP),
        P(None, TP, DP),
        P(None, DP, None, TP),
        P(None, DP, None, TP),
        P(None, DP, None, TP),
        P(None, DP, TP, None, None),
    )
    return jax.shard_map(
        local,
        mesh=finer,
        in_specs=placed,
        out_specs=(
            P(None, DP),
            P(None, DP, None, TP),
            P(None, DP, None, TP),
            P(None, DP, None, TP),
            P(None, DP, TP, None, None),
        ),
        check_vma=False,
    )
```
